256 devices in a mesh: ep: 128 (over z, y, x), tp: 2 (over core).
Axes of the slice: x: 4, y: 4, z: 8, core: 2. Of those that a mesh axis runs over, the one named last changes fastest.
Arguments:
- tokens: bfloat16 [1024, 2048], P('ep'), may hold values from -6 to 6
- first_gain: bfloat16 [2048], replicated, may hold values from 0.099609375 to 1.8984375
- query_weight: bfloat16 [2048, 256], P(None, 'tp'), may hold values from -0.125 to 0.125
- key_weight: bfloat16 [2048, 256], P(None, 'tp'), may hold values from -0.125 to 0.125
- value_weight: bfloat16 [2048, 512], P(None, 'tp'), may hold values from -0.125 to 0.125
- decay_down: bfloat16 [2048, 16], replicated, may hold values from -0.125 to 0.125
- decay_up: bfloat16 [16, 256], P(None, 'tp'), may hold values from -5 to 5
- decay_bias: float32 [256], P('tp'), may hold values from -12 to 4
- head_gain: bfloat16 [256], replicated, may hold values from 0.099609375 to 1.8984375
- recurrent_state: float32 [1024, 2, 128, 256], P('ep', 'tp'), may hold values from -6 to 6
- out_weight: bfloat16 [512, 2048], P('tp'), may hold values from -0.25 to 0.25
- second_gain: bfloat16 [2048], replicated, may hold values from 0.099609375 to 1.8984375
- expert_ids: int32 [1024, 6], P('ep'), may hold values from 0 to 127, all different within a row; in each aligned block of 8 rows (0 to 7, 8 to 15, ...) at most 2 rows name the same one
- route_weights: float32 [1024, 6], P('ep'), may hold values from 0.1 to 1
- expert_gate: bfloat16 [128, 2048, 256], P('ep', None, 'tp'), may hold values from -0.125 to 0.125
- expert_up: bfloat16 [128, 2048, 256], P('ep', None, 'tp'), may hold values from -0.125 to 0.125
- expert_down: bfloat16 [128, 256, 2048], P('ep', 'tp'), may hold values from -0.375 to 0.375
- dense_gate: bfloat16 [2048, 512], P('ep', 'tp'), may hold values from -0.5 to 0.5
- dense_up: bfloat16 [2048, 512], P('ep', 'tp'), may hold values from -0.5 to 0.5
- dense_down: bfloat16 [512, 2048], P('tp', 'ep'), may hold values from -0.25 to 0.25
- branch_gate: bfloat16 [2048], replicated, may hold values from -0.125 to 0.125
Outputs:
- layer_out: bfloat16 [1024, 2048], P('ep', 'tp')
The draws below stay inside these ranges and needn't reach their ends.
Inputs may be any that keep to these rules, and one draw needn't show every extreme that they name: `expert_ids`: each row names 6 different experts. Within the 8 rows of one index of ep no expert is named by more than 2 rows, a bound that some block reaches.
All inputs are finite; a program needn't handle non-finite values.
Results may differ from the reference program's by a relative error of at most 0.015.
Values may be sent and summed in bfloat16 or wider, within the bound.
No kernel may reach another device: no remote copies, remote signals or barrier semaphores. Data moves between devices by JAX's collectives and lax.ppermute only.
A program may use at most 128 MiB of HBM per device.

```python
import math
import jax
import jax.numpy as jnp
import numpy as np
from jax import lax

D = 2048
HEADS = 2
DK = 128
DV = 256
RANK = 16
FE = 256
FD = 512
TOPK = 6
SEQ_DEV = 8
SEQS = 1024
EXPERTS = 128
CAP = 2
KW = 256
VW = 512
N_EP = 128
N_TP = 2


def with_spikes(values, own_key, source, target, shards_of, factor):
    owner, partner = [(jnp.arange(values.shape[dim]) // (values.shape[dim] // shards_of)).reshape([-1 if axis == dim else 1 for axis in range(values.ndim)]) for dim in (source, target)]
    chosen = jax.random.permutation(own_key, shards_of)[partner]
    strong = (owner == chosen) | (owner == (partner + shards_of // 2) % shards_of)
    return jnp.where(strong, factor * values, values)


def block_scale(stream_key, extent, shards, low, high):
    def one(position, parts):
        draws = jax.random.uniform(jax.random.fold_in(jax.random.fold_in(stream_key, 6), position), (parts,), jnp.float32, low / len(shards), high / len(shards))
        return jnp.repeat(jnp.exp(draws), extent[position] // parts).reshape((-1,) + (1,) * (len(extent) - position - 1))

    loudness = one(*shards[0])
    for cut in shards[1:]:
        loudness = loudness * one(*cut)
    return loudness


def routed_block(stream_key, own, number, rows, amount, top, limit, skew):
    order = jax.random.permutation(stream_key, amount)
    heavy_load, ordinary = portions_of(amount, rows * top, limit, skew, True), portions_of(amount, rows * top, limit, skew, False)
    places = jnp.arange(amount)

    def named(sizes, rotation):
        used = int((sizes > 0).sum())
        fixed = max(1, used // 4)
        moved = fixed + (places - fixed + rotation * (used - fixed)) % max(1, amount - fixed)
        return jnp.zeros((amount,), jnp.int32).at[order[jnp.where(places < fixed, places, moved)]].set(jnp.asarray(sizes, jnp.int32))

    sizes = jnp.where(number % 4 == 0, named(heavy_load, number // 4), named(ordinary, number - number // 4 - 1))
    mixed = jax.random.permutation(jax.random.fold_in(own, 3), amount)
    source_of, receiver = mixed[0:amount // 2 * 2:2], mixed[1:amount // 2 * 2:2]
    margin = jnp.minimum(sizes[source_of] - 1, limit - sizes[receiver]) // 2
    margin = jnp.where((source_of == order[0]) | (receiver == order[0]) | (sizes[receiver] == 0), 0, jnp.maximum(margin, 0))
    moved = jax.random.randint(jax.random.fold_in(own, 4), (amount // 2,), 0, 1 << 20) % (margin + 1)
    sizes = sizes.at[source_of].add(-moved).at[receiver].add(moved)
    labels = jnp.searchsorted(jnp.cumsum(sizes), jnp.arange(rows * top), side="right").astype(jnp.int32)
    listing = labels.reshape(top, rows).T
    listing = listing[jax.random.permutation(jax.random.fold_in(own, 1), rows)]
    rotation = jax.random.randint(jax.random.fold_in(own, 2), (rows, 1), 0, top)
    return jnp.take_along_axis(listing, (jnp.arange(top)[None, :] + rotation) % top, axis=1)


def portions_of(number_of, total, limit, skew, full):
    weights = [(1 << 20) // math.isqrt(rank ** skew) + 1 for rank in range(1, number_of + 1)]
    largest = limit if full else min(limit, max(-(-total // number_of), total * weights[0] // sum(weights)))
    least = 1 if total - largest >= number_of - 1 else 0
    counts, rest = [largest] + [least] * (number_of - 1), total - largest - least * (number_of - 1)
    while rest > 0:
        candidates = [i for i in range(1, number_of) if counts[i] < largest] or [i for i in range(1, number_of) if counts[i] < limit]
        whole, remaining = sum([weights[i] for i in candidates]), rest
        for i in candidates:
            addition = min(limit - counts[i], max(1, remaining * weights[i] // whole), rest)
            counts[i] = counts[i] + addition
            rest = rest - addition
    return np.array(counts)


def normal_values(stream_key, dims, scale, reach, cuts=(), kind=jnp.bfloat16):
    drawn = jax.random.normal(stream_key, dims, jnp.float32) * scale
    if len(cuts) > 0:
        drawn = block_scale(stream_key, dims, cuts, -0.22, 0.18) * drawn
    return jnp.clip(drawn, min=-reach, max=reach).astype(kind)


def gaussian_with(rng, dims, spread, most, pieces, heavy, held_as=jnp.bfloat16):
    values = spread * jax.random.normal(rng, dims, jnp.float32)
    if pieces:
        values = values * block_scale(rng, dims, pieces, -0.22, 0.18)
    return jnp.clip(with_spikes(values, jax.random.fold_in(rng, 3), *heavy), -most, most).astype(held_as)


def setup_inputs(seed: int = 0) -> dict:
    streams_of = jax.random.split(jax.random.key(seed), 22)
    tokens = normal_values(streams_of[0], (SEQS, D), 1.0, 6.0, ((0, 128),))
    first_gain = jnp.clip(1.0 + 0.18 * jax.random.normal(streams_of[1], (D,), jnp.float32), 0.099609375, 1.8984375).astype(jnp.bfloat16)
    query_weight = normal_values(streams_of[2], (D, KW), D ** -0.5, 0.125, ((1, 2),))
    key_weight = normal_values(streams_of[3], (D, KW), D ** -0.5, 0.125, ((1, 2),))
    value_weight = normal_values(streams_of[4], (D, VW), D ** -0.5, 0.125, ((1, 2),))
    decay_down = normal_values(streams_of[5], (D, RANK), D ** -0.5, 0.125)
    decay_up = normal_values(streams_of[6], (RANK, KW), 1.0, 5.0, ((1, 2),))
    decay_bias = jnp.clip(-12.0 + 16.0 * jax.random.uniform(streams_of[7], (KW,), jnp.float32) ** block_scale(streams_of[7], (KW,), ((0, 2),), -0.2, 0.2), -12.0, 4.0)
    head_gain = jnp.clip(1.0 + 0.18 * jax.random.normal(streams_of[8], (DV,), jnp.float32), 0.099609375, 1.8984375).astype(jnp.bfloat16)
    recurrent_state = normal_values(streams_of[9], (SEQS, HEADS, DK, DV), 1.0, 6.0, ((0, 128), (1, 2)), jnp.float32)
    out_weight = normal_values(streams_of[10], (VW, D), VW ** -0.5, 0.25, ((0, 2),))
    second_gain = jnp.clip(1.0 + 0.18 * jax.random.normal(streams_of[11], (D,), jnp.float32), 0.099609375, 1.8984375).astype(jnp.bfloat16)
    expert_ids_keys = jax.random.split(jax.random.fold_in(streams_of[12], 1), SEQS // SEQ_DEV)
    expert_ids_turns = jax.random.permutation(jax.random.fold_in(streams_of[12], 3), SEQS // SEQ_DEV)
    expert_ids = jax.vmap(lambda own, number: routed_block(jax.random.fold_in(streams_of[12], 2), own, number, SEQ_DEV, EXPERTS, TOPK, CAP, 2))(expert_ids_keys, expert_ids_turns).reshape((SEQS, TOPK))
    route_weights = jnp.clip(jnp.exp(math.log(1.0) - 2.3025851 * jax.random.uniform(streams_of[13], (SEQS, TOPK), jnp.float32) ** block_scale(streams_of[13], (SEQS, TOPK), ((0, 128),), -0.2, 0.2)), 0.1, 1.0)
    expert_gate = normal_values(streams_of[14], (EXPERTS, D, FE), D ** -0.5, 0.125, ((0, 128), (2, 2)))
    expert_up = normal_values(streams_of[15], (EXPERTS, D, FE), D ** -0.5, 0.125, ((0, 128), (2, 2)))
    expert_down = normal_values(streams_of[16], (EXPERTS, FE, D), FE ** -0.5, 0.375, ((0, 128), (1, 2)))
    dense_gate = gaussian_with(streams_of[17], (D, FD), D ** -0.5, 0.5, ((0, 128), (1, 2)), (0, 1, 128, 5.5))
    dense_up = gaussian_with(streams_of[18], (D, FD), D ** -0.5, 0.5, ((0, 128), (1, 2)), (0, 1, 128, 5.5))
    dense_down = normal_values(streams_of[19], (FD, D), FD ** -0.5, 0.25, ((0, 2), (1, 128)))
    branch_gate = normal_values(streams_of[20], (D,), D ** -0.5, 0.125)
    return dict(tokens=tokens, first_gain=first_gain, query_weight=query_weight, key_weight=key_weight, value_weight=value_weight, decay_down=decay_down, decay_up=decay_up, decay_bias=decay_bias, head_gain=head_gain, recurrent_state=recurrent_state, out_weight=out_weight, second_gain=second_gain, expert_ids=expert_ids, route_weights=route_weights, expert_gate=expert_gate, expert_up=expert_up, expert_down=expert_down, dense_gate=dense_gate, dense_up=dense_up, dense_down=dense_down, branch_gate=branch_gate)


EPS = 1e-06

def rms_scale(values_in, gain):
    widened = values_in.astype(jnp.float32)
    return widened * lax.rsqrt(lax.optimization_barrier(jnp.mean(widened * widened, axis=-1, keepdims=True)) + EPS) * gain.astype(jnp.float32)

def round_half(values_in):
    return lax.optimization_barrier(values_in.astype(jnp.bfloat16)).astype(jnp.float32)

def reference(tokens, first_gain, query_weight, key_weight, value_weight, decay_down, decay_up, decay_bias, head_gain, recurrent_state, out_weight, second_gain, expert_ids, route_weights, expert_gate, expert_up, expert_down, dense_gate, dense_up, dense_down, branch_gate):
    seqs = tokens.shape[0]
    normed = rms_scale(tokens, first_gain).astype(jnp.bfloat16)
    query = jnp.dot(normed, query_weight, preferred_element_type=jnp.float32).reshape(seqs, HEADS, DK) * DK ** (-0.5)
    keys = jnp.dot(normed, key_weight, preferred_element_type=jnp.float32).reshape(seqs, HEADS, DK)
    values = jnp.dot(normed, value_weight, preferred_element_type=jnp.float32).reshape(seqs, HEADS, DV)
    decay_low = jnp.dot(normed, decay_down, preferred_element_type=jnp.float32).astype(jnp.bfloat16)
    decay_pre = jnp.dot(decay_low, decay_up, preferred_element_type=jnp.float32) + decay_bias
    log_decay = (jax.nn.log_sigmoid(decay_pre) / 16.0).reshape(seqs, HEADS, DK)
    new_state = jnp.exp(log_decay)[..., None] * recurrent_state + keys[..., None] * values[:, :, None, :]
    head_read = jnp.einsum('shk,shkv->shv', query, new_state, precision=lax.Precision.HIGHEST)
    head_read = head_read * lax.rsqrt(lax.optimization_barrier(jnp.mean(head_read * head_read, axis=-1, keepdims=True)) + EPS) * head_gain.astype(jnp.float32)
    heads_flat = head_read.astype(jnp.bfloat16).reshape(seqs, HEADS * DV)
    group_width = HEADS * DV // N_TP
    attention = jnp.zeros((seqs, D), jnp.float32)
    for group in range(N_TP):
        partial_value = jnp.dot(heads_flat[:, group * group_width:(group + 1) * group_width], out_weight[group * group_width:(group + 1) * group_width], preferred_element_type=jnp.float32)
        attention = attention + round_half(partial_value)
    residual = (tokens.astype(jnp.float32) + attention).astype(jnp.bfloat16)
    expert_in = rms_scale(residual, second_gain).astype(jnp.bfloat16)
    branch = jax.nn.sigmoid(jnp.dot(expert_in, branch_gate, preferred_element_type=jnp.float32))
    dense_pre = jnp.dot(expert_in, dense_gate, preferred_element_type=jnp.float32)
    dense_lift = jnp.dot(expert_in, dense_up, preferred_element_type=jnp.float32)
    dense_hidden = (jax.nn.silu(dense_pre) * dense_lift).astype(jnp.bfloat16)
    dense = jnp.dot(dense_hidden, dense_down, preferred_element_type=jnp.float32)
    rows_dev = seqs // N_EP
    choices_dev = rows_dev * TOPK
    blocked = expert_ids.reshape(N_EP, choices_dev)
    onehot = (blocked[..., None] == jnp.arange(EXPERTS, dtype=jnp.int32)[None, None, :]).astype(jnp.int32)
    lower = (jnp.arange(choices_dev, dtype=jnp.int32)[:, None] > jnp.arange(choices_dev, dtype=jnp.int32)[None, :]).astype(jnp.int32)
    earlier = jnp.einsum('rq,nqe->nre', lower, onehot)
    slot_ids = lax.optimization_barrier(jnp.sum(earlier * onehot, axis=-1)).astype(jnp.int32)
    source = jnp.arange(N_EP, dtype=jnp.int32)[:, None]
    target = ((blocked * N_EP + source) * CAP + slot_ids).astype(jnp.int32)
    token_of = (source * rows_dev + jnp.arange(choices_dev, dtype=jnp.int32)[None, :] // TOPK).astype(jnp.int32)
    table = jnp.full((EXPERTS * N_EP * CAP,), -1, jnp.int32).at[target.reshape(-1)].set(token_of.reshape(-1))
    table = table.reshape(EXPERTS, N_EP * CAP)
    hidden_group = FE // N_TP

    def run_expert(operands):
        index, weight_gate, weight_up, weight_down = operands
        live = index >= 0
        gathered = jnp.where(live[:, None], expert_in[jnp.maximum(index, 0)], jnp.zeros((), jnp.bfloat16))
        gate_pre = jnp.dot(gathered, weight_gate, preferred_element_type=jnp.float32)
        up_pre = jnp.dot(gathered, weight_up, preferred_element_type=jnp.float32)
        activated = (jax.nn.silu(gate_pre) * up_pre).astype(jnp.bfloat16)
        summed = jnp.zeros((gathered.shape[0], D), jnp.float32)
        for group in range(N_TP):
            partial_value = jnp.dot(activated[:, group * hidden_group:(group + 1) * hidden_group], weight_down[group * hidden_group:(group + 1) * hidden_group], preferred_element_type=jnp.float32)
            summed = summed + round_half(partial_value)
        return summed.astype(jnp.bfloat16)
    results = lax.map(run_expert, (table, expert_gate, expert_up, expert_down))
    picked = results.reshape(EXPERTS * N_EP * CAP, D)[target.reshape(seqs, TOPK)]
    shares = route_weights / lax.optimization_barrier(jnp.sum(route_weights, axis=-1, keepdims=True))
    routed = lax.optimization_barrier(jnp.sum(shares[..., None] * picked.astype(jnp.float32), axis=1))
    layer_out = residual.astype(jnp.float32) + routed + branch[:, None] * dense
    return layer_out.astype(jnp.bfloat16)
```

```python
import jax
import jax.numpy as jnp
from jax import lax
from jax.sharding import Mesh
from jax.sharding import PartitionSpec as P

DK = 128
DV = 256
TOPK = 6
EP = ("ep_0", "ep_1", "ep_2")


EPS = 1e-06


SWAP = [(0, 1), (1, 0)]


def swapped(array):
    return lax.ppermute(array, "tp", SWAP)


def half_of(array, index, dim):
    width = array.shape[dim] // 2
    return lax.dynamic_slice_in_dim(array, index * width, width, dim)


def exchanged(array, axis):
    return lax.all_to_all(array, axis, split_axis=0, concat_axis=0, tiled=True)


def rms_scale(values_in, gain):
    widened = values_in.astype(jnp.float32)
    return (
        widened
        * lax.rsqrt(jnp.mean(widened * widened, axis=-1, keepdims=True) + EPS)
        * gain.astype(jnp.float32)
    )


def shards(
    tokens,
    first_gain,
    query_weight,
    key_weight,
    value_weight,
    decay_down,
    decay_up,
    decay_bias,
    head_gain,
    recurrent_state,
    out_weight,
    second_gain,
    expert_ids,
    route_weights,
    expert_gate,
    expert_up,
    expert_down,
    dense_gate,
    dense_up,
    dense_down,
    branch_gate,
):
    rows_dev, width = tokens.shape
    core = lax.axis_index("tp")
    lines = lax.axis_size("ep_0")
    experts = lax.axis_size(EP)
    rows_own, hidden = dense_gate.shape
    units = hidden // lines
    packed = jnp.stack([dense_gate, dense_up, dense_down.T], axis=1)
    packed = packed.reshape(rows_own, 3, lines, units).transpose(2, 0, 1, 3)
    packed = packed.reshape(lines, 1, rows_own, 3 * units)
    packed = jnp.broadcast_to(packed, (lines, experts // lines, rows_own, 3 * units))
    dense_weights = exchanged(packed.reshape(experts, rows_own, 3 * units), EP).reshape(
        width, 3 * units
    )

    normed = rms_scale(tokens, first_gain).astype(jnp.bfloat16)
    query = jnp.dot(normed, query_weight, preferred_element_type=jnp.float32) * DK ** (-0.5)
    keys = jnp.dot(normed, key_weight, preferred_element_type=jnp.float32)
    values = jnp.dot(normed, value_weight, preferred_element_type=jnp.float32)
    decay_low = jnp.dot(normed, decay_down, preferred_element_type=jnp.float32).astype(jnp.bfloat16)
    decay_pre = jnp.dot(decay_low, decay_up, preferred_element_type=jnp.float32) + decay_bias
    decay = jnp.exp(jax.nn.log_sigmoid(decay_pre) / 16.0)
    head_read = (
        jnp.sum((query * decay)[:, :, None] * recurrent_state[:, 0], axis=1)
        + jnp.sum(query * keys, axis=1, keepdims=True) * values
    )
    head_read = (
        head_read
        * lax.rsqrt(jnp.mean(head_read * head_read, axis=-1, keepdims=True) + EPS)
        * head_gain.astype(jnp.float32)
    )
    partial_value = jnp.dot(
        head_read.astype(jnp.bfloat16), out_weight, preferred_element_type=jnp.float32
    ).astype(jnp.bfloat16)
    attention = partial_value.astype(jnp.float32) + swapped(partial_value).astype(jnp.float32)
    residual = (tokens.astype(jnp.float32) + attention).astype(jnp.bfloat16)
    expert_in = rms_scale(residual, second_gain).astype(jnp.bfloat16)
    branch = jax.nn.sigmoid(jnp.dot(expert_in, branch_gate, preferred_element_type=jnp.float32))

    capacity = max(2, 2 * rows_dev * TOPK // experts)
    flat_ids = expert_ids.reshape(-1)
    choices_dev = flat_ids.shape[0]
    onehot = (flat_ids[:, None] == jnp.arange(experts, dtype=jnp.int32)[None, :]).astype(
        jnp.float32
    )
    lower = (
        jnp.arange(choices_dev, dtype=jnp.int32)[:, None]
        > jnp.arange(choices_dev, dtype=jnp.int32)[None, :]
    ).astype(jnp.float32)
    earlier = jnp.dot(lower, onehot, precision=lax.Precision.HIGHEST)
    slot_ids = jnp.sum(earlier * onehot, axis=1)
    slot_hot = (slot_ids[:, None] == jnp.arange(capacity, dtype=jnp.float32)[None, :]).astype(
        jnp.float32
    )
    placing = (onehot[:, :, None] * slot_hot[:, None, :]).reshape(choices_dev, experts * capacity)
    owners = (
        jnp.arange(choices_dev, dtype=jnp.int32)[:, None] // TOPK
        == jnp.arange(rows_dev, dtype=jnp.int32)[None, :]
    ).astype(jnp.float32)
    send_map = jnp.einsum("rs,rt->st", placing, owners).astype(jnp.bfloat16)
    shares = route_weights / jnp.sum(route_weights, axis=-1, keepdims=True)
    weighing = jnp.einsum(
        "rt,rs->ts", owners, placing * shares.reshape(-1)[:, None], precision=lax.Precision.HIGHEST
    )

    line_in = exchanged(
        jnp.broadcast_to(expert_in[None], (lines, rows_dev, width)), "ep_0"
    ).reshape(lines * rows_dev, width)
    outgoing = (
        jnp.dot(send_map, half_of(expert_in, core, 1), preferred_element_type=jnp.float32)
        .astype(jnp.bfloat16)
        .reshape(experts, capacity, -1)
    )
    arrived = exchanged(outgoing, EP)
    paired = jnp.dot(line_in, dense_weights, preferred_element_type=jnp.float32)
    line_hidden = (
        jax.nn.silu(paired[:, :units]) * paired[:, units : 2 * units]
    ).astype(jnp.bfloat16)
    line_part = lax.dot_general(
        jnp.pad(line_hidden, ((0, 0), (2 * units, 0))),
        dense_weights,
        (((1,), (1,)), ((), ())),
        preferred_element_type=jnp.float32,
    ).astype(jnp.bfloat16)
    line_sum = half_of(line_part, core, 1).astype(jnp.float32) + swapped(
        half_of(line_part, 1 - core, 1)
    ).astype(jnp.float32)
    dense = (
        exchanged(line_sum.astype(jnp.bfloat16).reshape(lines, rows_dev, width // 2), "ep_0")
        .astype(jnp.float32)
        .sum(axis=0)
    )

    mine = arrived.reshape(experts * capacity, -1)
    theirs = swapped(mine)
    gate, up, down = expert_gate[0], expert_up[0], expert_down[0]
    gate_pre = jnp.dot(
        mine, half_of(gate, core, 0), preferred_element_type=jnp.float32
    ) + jnp.dot(theirs, half_of(gate, 1 - core, 0), preferred_element_type=jnp.float32)
    up_pre = jnp.dot(
        mine, half_of(up, core, 0), preferred_element_type=jnp.float32
    ) + jnp.dot(theirs, half_of(up, 1 - core, 0), preferred_element_type=jnp.float32)
    activated = (jax.nn.silu(gate_pre) * up_pre).astype(jnp.bfloat16)
    for_them = jnp.dot(
        activated, half_of(down, 1 - core, 1), preferred_element_type=jnp.float32
    ).astype(jnp.bfloat16)
    for_me = jnp.dot(
        activated, half_of(down, core, 1), preferred_element_type=jnp.float32
    ).astype(jnp.bfloat16)
    summed = (for_me.astype(jnp.float32) + swapped(for_them).astype(jnp.float32)).astype(
        jnp.bfloat16
    )
    came_back = exchanged(summed.reshape(experts, capacity, -1), EP)
    routed = jnp.dot(
        weighing,
        came_back.reshape(experts * capacity, -1).astype(jnp.float32),
        precision=lax.Precision.HIGHEST,
    )
    own_half = half_of(residual, core, 1).astype(jnp.float32)
    return (own_half + routed + branch[:, None] * dense).astype(jnp.bfloat16)


def solution(mesh):
    split = Mesh(mesh.devices.reshape(8, 4, 4, mesh.shape["tp"]), ("ep_0", "ep_1", "ep_2", "tp"))
    placed = (
        P(EP, None),
        P(),
        P(None, "tp"),
        P(None, "tp"),
        P(None, "tp"),
        P(),
        P(None, "tp"),
        P("tp"),
        P(),
        P(EP, "tp", None, None),
        P("tp", None),
        P(),
        P(EP, None),
        P(EP, None),
        P(EP, None, "tp"),
        P(EP, None, "tp"),
        P(EP, "tp", None),
        P(EP, "tp"),
        P(EP, "tp"),
        P("tp", EP),
        P(),
    )
    return jax.shard_map(
        shards, mesh=split, in_specs=placed, out_specs=P(EP, "tp"), check_vma=False
    )
```

```python
import jax
import jax.numpy as jnp
from jax import lax
from jax.sharding import Mesh
from jax.sharding import PartitionSpec as P

DK = 128
DV = 256
TOPK = 6
EP = ("ep_0", "ep_1", "ep_2")
PLANE = ("ep_1", "ep_2")
CAP = 2


EPS = 1e-06


SWAP = [(0, 1), (1, 0)]


def swapped(array):
    return lax.ppermute(array, "tp", SWAP)


def half_of(array, index, dim):
    width = array.shape[dim] // 2
    return lax.dynamic_slice_in_dim(array, index * width, width, dim)


def exchanged(array, axis):
    return lax.all_to_all(array, axis, split_axis=0, concat_axis=0, tiled=True)


def rms_scale(values_in, gain):
    widened = values_in.astype(jnp.float32)
    return (
        widened
        * lax.rsqrt(jnp.mean(widened * widened, axis=-1, keepdims=True) + EPS)
        * gain.astype(jnp.float32)
    )


def shards(
    tokens,
    first_gain,
    query_weight,
    key_weight,
    value_weight,
    decay_down,
    decay_up,
    decay_bias,
    head_gain,
    recurrent_state,
    out_weight,
    second_gain,
    expert_ids,
    route_weights,
    expert_gate,
    expert_up,
    expert_down,
    dense_gate,
    dense_up,
    dense_down,
    branch_gate,
):
    rows_dev, width = tokens.shape
    core = lax.axis_index("tp")
    lines = lax.axis_size("ep_0")
    plane = lax.axis_size(PLANE)
    experts = lines * plane
    half = width // 2
    rows_own, hidden = dense_gate.shape
    units = hidden // lines
    packed = jnp.stack([dense_gate, dense_up, dense_down.T], axis=1)
    packed = packed.reshape(rows_own, 3, lines, units).transpose(2, 0, 1, 3)
    packed = packed.reshape(lines, rows_own, 3 * units)
    shares = route_weights / jnp.sum(route_weights, axis=-1, keepdims=True)
    named = (expert_ids[:, :, None] == jnp.arange(experts, dtype=jnp.int32)).astype(jnp.float32)
    chosen = named.sum(axis=1)
    earlier = jnp.cumsum(chosen, axis=0) - chosen
    place = chosen * (1.0 + earlier)
    share = (named * shares[:, :, None]).sum(axis=1)
    share_high = share.astype(jnp.bfloat16)
    share_low = (share - share_high.astype(jnp.float32)).astype(jnp.bfloat16)

    def by_line(array):
        return array.astype(jnp.bfloat16).reshape(rows_dev, lines, plane).transpose(1, 0, 2)

    side = jnp.concatenate(
        [
            packed[:, :rows_dev],
            by_line(place),
            by_line(share_high),
            packed[:, rows_dev:],
            by_line(share_low),
            jnp.zeros((lines, rows_dev, plane), jnp.bfloat16),
        ],
        axis=2,
    )

    normed = rms_scale(tokens, first_gain).astype(jnp.bfloat16)
    query = jnp.dot(normed, query_weight, preferred_element_type=jnp.float32) * DK ** (-0.5)
    keys = jnp.dot(normed, key_weight, preferred_element_type=jnp.float32)
    values = jnp.dot(normed, value_weight, preferred_element_type=jnp.float32)
    decay_low = jnp.dot(normed, decay_down, preferred_element_type=jnp.float32).astype(jnp.bfloat16)
    decay_pre = jnp.dot(decay_low, decay_up, preferred_element_type=jnp.float32) + decay_bias
    decay = jnp.exp(jax.nn.log_sigmoid(decay_pre) / 16.0)
    head_read = (
        jnp.sum((query * decay)[:, :, None] * recurrent_state[:, 0], axis=1)
        + jnp.sum(query * keys, axis=1, keepdims=True) * values
    )
    head_read = (
        head_read
        * lax.rsqrt(jnp.mean(head_read * head_read, axis=-1, keepdims=True) + EPS)
        * head_gain.astype(jnp.float32)
    )
    partial_value = jnp.dot(
        head_read.astype(jnp.bfloat16), out_weight, preferred_element_type=jnp.float32
    ).astype(jnp.bfloat16)
    attention = partial_value.astype(jnp.float32) + swapped(partial_value).astype(jnp.float32)
    residual = (tokens.astype(jnp.float32) + attention).astype(jnp.bfloat16)
    expert_in = rms_scale(residual, second_gain).astype(jnp.bfloat16)

    first = jnp.concatenate(
        [jnp.broadcast_to(expert_in[None], (lines, rows_dev, width)), side], axis=2
    )
    line = exchanged(first, "ep_0").reshape(lines * rows_dev, width + 256)
    line_in = line[:, :width]
    line_place = line[:, width + 96 : width + 112]
    line_high = line[:, width + 112 : width + 128]
    line_low = line[:, width + 224 : width + 240]
    slots = plane * lines * CAP
    row = lax.broadcasted_iota(jnp.int32, (slots, lines * rows_dev), 0)
    col = lax.broadcasted_iota(jnp.int32, (slots, lines * rows_dev), 1)
    spread = (
        lax.broadcasted_iota(jnp.int32, (slots, plane), 0) // (lines * CAP)
        == lax.broadcasted_iota(jnp.int32, (slots, plane), 1)
    ).astype(jnp.bfloat16)

    def over_slots(array):
        return lax.dot_general(
            spread, array, (((1,), (1,)), ((), ())), preferred_element_type=jnp.float32
        )

    taken = (over_slots(line_place) == (1 + row % CAP).astype(jnp.float32)) & (
        row // CAP % lines == col // rows_dev
    )
    rows = jnp.dot(
        taken.astype(jnp.bfloat16), half_of(line_in, core, 1), preferred_element_type=jnp.float32
    ).astype(jnp.bfloat16)
    weights = line[:, width:].reshape(4, lines * rows_dev // 4, 256).transpose(1, 0, 2)
    weights = weights.reshape(1, lines * rows_dev // 4, half)
    second = jnp.concatenate(
        [
            rows.reshape(plane, lines * CAP, half),
            jnp.broadcast_to(weights, (plane, lines * rows_dev // 4, half)),
        ],
        axis=2,
    )
    arrived = exchanged(second, PLANE)
    mine = arrived[:, :, :half].reshape(slots, half)
    dense_weights = (
        arrived[:, :, half:]
        .reshape(plane, 2, rows_dev, 4, 2, 128)
        .transpose(3, 1, 0, 4, 2, 5)
        .reshape(width, 128)
    )

    theirs = swapped(mine)
    gate, up, down = expert_gate[0], expert_up[0], expert_down[0]
    gate_pre = jnp.dot(
        mine, half_of(gate, core, 0), preferred_element_type=jnp.float32
    ) + jnp.dot(theirs, half_of(gate, 1 - core, 0), preferred_element_type=jnp.float32)
    up_pre = jnp.dot(
        mine, half_of(up, core, 0), preferred_element_type=jnp.float32
    ) + jnp.dot(theirs, half_of(up, 1 - core, 0), preferred_element_type=jnp.float32)
    activated = (jax.nn.silu(gate_pre) * up_pre).astype(jnp.bfloat16)
    for_them = jnp.dot(
        activated, half_of(down, 1 - core, 1), preferred_element_type=jnp.float32
    ).astype(jnp.bfloat16)
    for_me = jnp.dot(
        activated, half_of(down, core, 1), preferred_element_type=jnp.float32
    ).astype(jnp.bfloat16)
    summed = (for_me.astype(jnp.float32) + swapped(for_them).astype(jnp.float32)).astype(
        jnp.bfloat16
    )
    summed, dense_weights = lax.optimization_barrier((summed, dense_weights))
    with jax.named_scope("return"):
        came_back = exchanged(summed.reshape(plane, lines * CAP, half), PLANE)
    with jax.named_scope("dense"):
        branch = jax.nn.sigmoid(jnp.dot(line_in, branch_gate, preferred_element_type=jnp.float32))
        paired = jnp.dot(line_in, dense_weights, preferred_element_type=jnp.float32)
        line_hidden = (jax.nn.silu(paired[:, :units]) * paired[:, units : 2 * units]).astype(
            jnp.bfloat16
        )
        line_part = lax.dot_general(
            jnp.pad(line_hidden, ((0, 0), (2 * units, 128 - 3 * units))),
            dense_weights,
            (((1,), (1,)), ((), ())),
            preferred_element_type=jnp.float32,
        ).astype(jnp.bfloat16)
        dense = branch[:, None] * (
            half_of(line_part, core, 1).astype(jnp.float32)
            + swapped(half_of(line_part, 1 - core, 1)).astype(jnp.float32)
        )
        weighing = jnp.where(taken, over_slots(line_high) + over_slots(line_low), 0.0)
        weigh_high = weighing.astype(jnp.bfloat16)
        weigh_low = (weighing - weigh_high.astype(jnp.float32)).astype(jnp.bfloat16)

    def combined(part):
        return lax.dot_general(
            part,
            came_back.reshape(slots, half),
            (((0,), (0,)), ((), ())),
            preferred_element_type=jnp.float32,
        )

    third = (combined(weigh_high) + combined(weigh_low) + dense).astype(jnp.bfloat16)
    parts = exchanged(third.reshape(lines, rows_dev, half), "ep_0")
    own_half = half_of(residual, core, 1).astype(jnp.float32)
    return (own_half + parts.astype(jnp.float32).sum(axis=0)).astype(jnp.bfloat16)


def solution(mesh):
    split = Mesh(mesh.devices.reshape(8, 4, 4, mesh.shape["tp"]), ("ep_0", "ep_1", "ep_2", "tp"))
    placed = (
        P(EP, None),
        P(),
        P(None, "tp"),
        P(None, "tp"),
        P(None, "tp"),
        P(),
        P(None, "tp"),
        P("tp"),
        P(),
        P(EP, "tp", None, None),
        P("tp", None),
        P(),
        P(EP, None),
        P(EP, None),
        P(EP, None, "tp"),
        P(EP, None, "tp"),
        P(EP, "tp", None),
        P(EP, "tp"),
        P(EP, "tp"),
        P("tp", EP),
        P(),
    )
    return jax.shard_map(
        shards, mesh=split, in_specs=placed, out_specs=P(EP, "tp"), check_vma=False
    )
```

```python
import jax
import jax.numpy as jnp
from jax import lax
from jax.sharding import Mesh
from jax.sharding import PartitionSpec as P


DK = 128
EP = ("ep_0", "ep_1", "ep_2")
PLANE = ("ep_1", "ep_2")
CAP = 2


EPS = 1e-06


SWAP = [(0, 1), (1, 0)]


def swapped(array):
    return lax.ppermute(array, "tp", SWAP)


def half_of(array, index, dim):
    width = array.shape[dim] // 2
    return lax.dynamic_slice_in_dim(array, index * width, width, dim)


def exchanged(array, axis):
    return lax.all_to_all(array, axis, split_axis=0, concat_axis=0, tiled=True)


def rms_scale(values_in, gain):
    widened = values_in.astype(jnp.float32)
    return (
        widened
        * lax.rsqrt(jnp.mean(widened * widened, axis=-1, keepdims=True) + EPS)
        * gain.astype(jnp.float32)
    )


def shards(
    tokens,
    first_gain,
    query_weight,
    key_weight,
    value_weight,
    decay_down,
    decay_up,
    decay_bias,
    head_gain,
    recurrent_state,
    out_weight,
    second_gain,
    expert_ids,
    route_weights,
    expert_gate,
    expert_up,
    expert_down,
    dense_gate,
    dense_up,
    dense_down,
    branch_gate,
):
    rows_dev, width = tokens.shape
    core = lax.axis_index("tp")
    lines = lax.axis_size("ep_0")
    plane = lax.axis_size(PLANE)
    experts = lines * plane
    half = width // 2
    rows_own, hidden = dense_gate.shape
    units = hidden // lines
    packed = jnp.stack([dense_gate, dense_up, dense_down.T], axis=1)
    packed = packed.reshape(rows_own, 3, lines, units).transpose(2, 0, 1, 3)
    packed = packed.reshape(lines, rows_own, 3 * units)
    shares = route_weights / jnp.sum(route_weights, axis=-1, keepdims=True)
    named = (expert_ids[:, :, None] == jnp.arange(experts, dtype=jnp.int32)).astype(jnp.float32)
    chosen = named.sum(axis=1)
    earlier = jnp.cumsum(chosen, axis=0) - chosen
    place = chosen * (1.0 + earlier)
    share = (named * shares[:, :, None]).sum(axis=1)
    share_high = share.astype(jnp.bfloat16)
    share_low = (share - share_high.astype(jnp.float32)).astype(jnp.bfloat16)

    def by_line(array):
        return array.astype(jnp.bfloat16).reshape(rows_dev, lines, plane).transpose(1, 0, 2)

    side = jnp.concatenate(
        [
            packed[:, :rows_dev],
            by_line(place),
            by_line(share_high),
            packed[:, rows_dev:],
            by_line(share_low),
            jnp.zeros((lines, rows_dev, plane), jnp.bfloat16),
        ],
        axis=2,
    )

    normed = rms_scale(tokens, first_gain).astype(jnp.bfloat16)
    query = jnp.dot(normed, query_weight, preferred_element_type=jnp.float32) * DK ** (-0.5)
    keys = jnp.dot(normed, key_weight, preferred_element_type=jnp.float32)
    values = jnp.dot(normed, value_weight, preferred_element_type=jnp.float32)
    decay_low = jnp.dot(normed, decay_down, preferred_element_type=jnp.float32).astype(jnp.bfloat16)
    decay_pre = jnp.dot(decay_low, decay_up, preferred_element_type=jnp.float32) + decay_bias
    decay = jnp.exp(jax.nn.log_sigmoid(decay_pre) / 16.0)
    head_read = (
        jnp.sum((query * decay)[:, :, None] * recurrent_state[:, 0], axis=1)
        + jnp.sum(query * keys, axis=1, keepdims=True) * values
    )
    head_read = (
        head_read
        * lax.rsqrt(jnp.mean(head_read * head_read, axis=-1, keepdims=True) + EPS)
        * head_gain.astype(jnp.float32)
    )
    partial_value = jnp.dot(
        head_read.astype(jnp.bfloat16), out_weight, preferred_element_type=jnp.float32
    ).astype(jnp.bfloat16)
    attention = partial_value.astype(jnp.float32) + swapped(partial_value).astype(jnp.float32)
    residual = (tokens.astype(jnp.float32) + attention).astype(jnp.bfloat16)
    expert_in = rms_scale(residual, second_gain).astype(jnp.bfloat16)

    first = jnp.concatenate(
        [jnp.broadcast_to(half_of(expert_in, core, 1)[None], (lines, rows_dev, half)), side],
        axis=2,
    )
    first, gate, up, down = lax.optimization_barrier(
        (first, expert_gate[0], expert_up[0], expert_down[0])
    )
    line = exchanged(first, "ep_0")
    line = line.reshape(lines * rows_dev, half + 256)
    given = jnp.concatenate([half_of(gate, 1 - core, 0), half_of(up, 1 - core, 0)], axis=1)
    taken_in = swapped(given)
    taken_down = swapped(half_of(down, 1 - core, 1))
    inner = gate.shape[1]
    weights_in = jnp.concatenate(
        [half_of(gate, core, 0), taken_in[:, :inner], half_of(up, core, 0), taken_in[:, inner:]],
        axis=1,
    )
    weights_down = jnp.concatenate([half_of(down, core, 1), taken_down], axis=0)
    line_in = line[:, :half]
    line_place = line[:, half + 96 : half + 112]
    line_high = line[:, half + 112 : half + 128]
    line_low = line[:, half + 224 : half + 240]
    slots = plane * lines * CAP
    row = lax.broadcasted_iota(jnp.int32, (slots, lines * rows_dev), 0)
    col = lax.broadcasted_iota(jnp.int32, (slots, lines * rows_dev), 1)
    spread = (
        lax.broadcasted_iota(jnp.int32, (slots, plane), 0) // (lines * CAP)
        == lax.broadcasted_iota(jnp.int32, (slots, plane), 1)
    ).astype(jnp.bfloat16)

    def over_slots(array):
        return lax.dot_general(
            spread, array, (((1,), (1,)), ((), ())), preferred_element_type=jnp.float32
        )

    taken = (over_slots(line_place) == (1 + row % CAP).astype(jnp.float32)) & (
        row // CAP % lines == col // rows_dev
    )
    rows = jnp.dot(
        taken.astype(jnp.bfloat16), line_in, preferred_element_type=jnp.float32
    ).astype(jnp.bfloat16)
    weights = line[:, half:].reshape(4, lines * rows_dev // 4, 256).transpose(1, 0, 2)
    weights = weights.reshape(1, lines * rows_dev // 4, half)
    second = jnp.concatenate(
        [
            rows.reshape(plane, lines * CAP, half),
            jnp.broadcast_to(weights, (plane, lines * rows_dev // 4, half)),
        ],
        axis=2,
    )
    arrived = exchanged(second, PLANE)
    mine = arrived[:, :, :half].reshape(slots, half)
    dense_weights = (
        arrived[:, :, half:]
        .reshape(plane, 2, rows_dev, 4, 2, 128)
        .transpose(3, 1, 0, 4, 2, 5)
        .reshape(width, 128)
    )

    partial_in = jnp.dot(mine, weights_in, preferred_element_type=jnp.float32)
    blocks = [partial_in[:, k * inner : (k + 1) * inner] for k in (1, 0, 3, 2)]
    pre = partial_in + swapped(
        jnp.concatenate(blocks, axis=1).astype(jnp.bfloat16)
    ).astype(jnp.float32)
    activated = (jax.nn.silu(pre[:, : 2 * inner]) * pre[:, 2 * inner :]).astype(jnp.bfloat16)
    summed = jnp.dot(activated, weights_down, preferred_element_type=jnp.float32).astype(
        jnp.bfloat16
    )
    summed, dense_weights, line_in = lax.optimization_barrier((summed, dense_weights, line_in))
    came_back = exchanged(summed.reshape(plane, lines * CAP, half), PLANE)
    line_rest = swapped(line_in)
    pre_gate = jnp.dot(
        line_in, half_of(branch_gate, core, 0), preferred_element_type=jnp.float32
    ) + jnp.dot(line_rest, half_of(branch_gate, 1 - core, 0), preferred_element_type=jnp.float32)
    branch = jax.nn.sigmoid(pre_gate)
    paired = jnp.dot(
        line_in, half_of(dense_weights, core, 0), preferred_element_type=jnp.float32
    ) + jnp.dot(line_rest, half_of(dense_weights, 1 - core, 0), preferred_element_type=jnp.float32)
    line_hidden = (jax.nn.silu(paired[:, :units]) * paired[:, units : 2 * units]).astype(
        jnp.bfloat16
    )
    line_part = lax.dot_general(
        jnp.pad(line_hidden, ((0, 0), (2 * units, 128 - 3 * units))),
        dense_weights,
        (((1,), (1,)), ((), ())),
        preferred_element_type=jnp.float32,
    ).astype(jnp.bfloat16)
    dense = branch[:, None] * (
        half_of(line_part, core, 1).astype(jnp.float32)
        + swapped(half_of(line_part, 1 - core, 1)).astype(jnp.float32)
    )
    weighing = jnp.where(taken, over_slots(line_high) + over_slots(line_low), 0.0)
    weigh_high = weighing.astype(jnp.bfloat16)
    weigh_low = (weighing - weigh_high.astype(jnp.float32)).astype(jnp.bfloat16)

    def combined(part):
        return lax.dot_general(
            part,
            came_back.reshape(slots, half),
            (((0,), (0,)), ((), ())),
            preferred_element_type=jnp.float32,
        )

    third = (combined(weigh_high) + combined(weigh_low) + dense).astype(jnp.bfloat16)
    parts = exchanged(third.reshape(lines, rows_dev, half), "ep_0")
    own_half = half_of(residual, core, 1).astype(jnp.float32)
    return (own_half + parts.astype(jnp.float32).sum(axis=0)).astype(jnp.bfloat16)


def solution(mesh):
    split = Mesh(mesh.devices.reshape(8, 4, 4, mesh.shape["tp"]), ("ep_0", "ep_1", "ep_2", "tp"))
    placed = (
        P(EP, None),
        P(),
        P(None, "tp"),
        P(None, "tp"),
        P(None, "tp"),
        P(),
        P(None, "tp"),
        P("tp"),
        P(),
        P(EP, "tp", None, None),
        P("tp", None),
        P(),
        P(EP, None),
        P(EP, None),
        P(EP, None, "tp"),
        P(EP, None, "tp"),
        P(EP, "tp", None),
        P(EP, "tp"),
        P(EP, "tp"),
        P("tp", EP),
        P(),
    )
    return jax.shard_map(
        shards, mesh=split, in_specs=placed, out_specs=P(EP, "tp"), check_vma=False
    )
```

```python
import jax
import jax.numpy as jnp
from jax import lax
from jax.sharding import Mesh
from jax.sharding import PartitionSpec as P

from jax.experimental import pallas as pl
from jax.experimental.pallas import tpu as pltpu

DK = 128
TOPK = 6
EP = ("ep_0", "ep_1", "ep_2")
PLANE = ("ep_1", "ep_2")
CAP = 2


EPS = 1e-06


SWAP = [(0, 1), (1, 0)]


def swapped(array):
    return lax.ppermute(array, "tp", SWAP)


def half_of(array, index, dim):
    width = array.shape[dim] // 2
    return lax.dynamic_slice_in_dim(array, index * width, width, dim)


def exchanged(array, axis):
    return lax.all_to_all(array, axis, split_axis=0, concat_axis=0, tiled=True)


def rms_scale(values_in, gain):
    widened = values_in.astype(jnp.float32)
    return (
        widened
        * lax.rsqrt(jnp.mean(widened * widened, axis=-1, keepdims=True) + EPS)
        * gain.astype(jnp.float32)
    )


def dot(a, b, dims=((1,), (0,))):
    return lax.dot_general(a, b, (dims, ((), ())), preferred_element_type=jnp.float32)


FAR = pl.BlockSpec(memory_space=pl.ANY)
NEAR = pl.BlockSpec(memory_space=pltpu.VMEM)


def in_vmem(array):
    return pltpu.with_memory_space_constraint(array, pltpu.VMEM)


def placed_lanes(tile, lane, source, target, size):
    shift = (target - source) % 128
    turned = tile if shift == 0 else pltpu.roll(tile, shift, 1)
    return jnp.where((lane >= target) & (lane < target + size), turned, 0.0)


def attend(*refs):
    far, result, side, near, done = refs[:16], refs[16], refs[17], refs[18:34], refs[34]
    copies = [pltpu.make_async_copy(far[k], near[k], done.at[k]) for k in range(16)]
    for copy in copies:
        copy.start()
    (
        tokens, gain, query_weight, decay_down, key_weight, decay_up, decay_bias, value_weight,
        ids, weights, dense_gate, dense_up, dense_down, state, head_gain, out_weight,
    ) = near
    count = tokens.shape[0]
    copies[0].wait()
    copies[1].wait()
    normed = rms_scale(tokens[...], gain[...][None, :]).astype(jnp.bfloat16)
    copies[2].wait()
    query = dot(normed, query_weight[...]) * DK ** (-0.5)
    copies[3].wait()
    decay_low = dot(normed, decay_down[...], ((1,), (1,))).astype(jnp.bfloat16)
    copies[4].wait()
    keys = dot(normed, key_weight[...])
    copies[5].wait()
    copies[6].wait()
    decay_pre = dot(decay_low, decay_up[...]) + decay_bias[...][None, :]
    log_decay = jnp.minimum(decay_pre, 0.0) - jnp.log1p(jnp.exp(-jnp.abs(decay_pre)))
    columns = jnp.transpose(query * jnp.exp(log_decay / 16.0))
    copies[7].wait()
    values = dot(normed, value_weight[...])

    for k in range(8, 13):
        copies[k].wait()
    lane = lax.broadcasted_iota(jnp.int32, (8, 128), 1)
    line = lax.broadcasted_iota(jnp.int32, (8, 128), 0)
    shares = weights[...] / jnp.sum(weights[...], axis=1, keepdims=True)
    chosen = jnp.zeros((8, 128), jnp.float32)
    share = jnp.zeros((8, 128), jnp.float32)
    for k in range(TOPK):
        named = ids[:, k : k + 1] == lane
        chosen = chosen + jnp.where(named, 1.0, 0.0)
        share = share + jnp.where(named, shares[:, k : k + 1], 0.0)
    place = jnp.where(chosen > 0.0, 1.0, 0.0)
    for k in range(1, count):
        place = place + jnp.where(line >= k, pltpu.roll(chosen, k, 0), 0.0)
    place = place * chosen
    share_high = share.astype(jnp.bfloat16).astype(jnp.float32)
    share_low = share - share_high
    for z in range(8):
        tiles = []
        for part in range(2):
            tile = jnp.zeros((8, 128), jnp.float32)
            for m, matrix in enumerate((dense_gate, dense_up, dense_down)):
                start = 128 * (z // 4)
                piece = matrix[...].astype(jnp.float32)[8 * part : 8 * part + 8, start : start + 128]
                tile = tile + placed_lanes(piece, lane, 32 * (z % 4), 32 * m, 32)
            tiles.append(tile)
        tiles[0] = tiles[0] + placed_lanes(place, lane, 16 * z, 96, 16)
        tiles[0] = tiles[0] + placed_lanes(share_high, lane, 16 * z, 112, 16)
        tiles[1] = tiles[1] + placed_lanes(share_low, lane, 16 * z, 96, 16)
        side[z] = jnp.concatenate(tiles, axis=1).astype(jnp.bfloat16)

    copies[13].wait()
    read = [
        jnp.sum(columns[:, k : k + 1] * state[k], axis=0, keepdims=True) for k in range(count)
    ]
    head = jnp.concatenate(read, axis=0) + jnp.sum(query * keys, axis=1, keepdims=True) * values
    copies[14].wait()
    head = rms_scale(head, head_gain[...][None, :]).astype(jnp.bfloat16)
    copies[15].wait()
    result[...] = dot(head, out_weight[...]).astype(jnp.bfloat16)


def attended(*held):
    tokens = held[0]
    return pl.pallas_call(
        attend,
        out_shape=(
            pltpu.VMEM(tokens.shape, jnp.bfloat16),
            pltpu.VMEM((8, 8, 256), jnp.bfloat16),
        ),
        in_specs=[FAR] * 16,
        out_specs=(NEAR, NEAR),
        scratch_shapes=[pltpu.VMEM(a.shape, a.dtype) for a in held]
        + [pltpu.SemaphoreType.DMA((16,))],
        name="attend",
    )(*held)


def assemble(core, tokens, mine, theirs, gain, side, first, own, block, done):
    sides = pltpu.make_async_copy(side, first.at[:, :, pl.ds(1024, 256)], done.at[8])
    sides.start()
    both = mine[...].astype(jnp.float32) + theirs[...].astype(jnp.float32)
    residual = (tokens[...].astype(jnp.float32) + both).astype(jnp.bfloat16)
    normed = rms_scale(residual, gain[...][None, :])
    half = normed.shape[1] // 2
    first_half = core[0] == 0
    block[...] = jnp.where(first_half, normed[:, :half], normed[:, half:]).astype(jnp.bfloat16)
    copies = [
        pltpu.make_async_copy(block, first.at[z, :, pl.ds(0, 1024)], done.at[z]) for z in range(8)
    ]
    for copy in copies:
        copy.start()
    wide = residual.astype(jnp.float32)
    own[...] = jnp.where(first_half, wide[:, :half], wide[:, half:])
    for copy in copies:
        copy.wait()
    sides.wait()


def assembled(core, tokens, mine, theirs, gain, side):
    rows, width = tokens.shape
    return pl.pallas_call(
        assemble,
        out_shape=(
            jax.ShapeDtypeStruct((8, rows, width // 2 + 256), jnp.bfloat16),
            pltpu.VMEM((rows, width // 2), jnp.float32),
        ),
        in_specs=[pl.BlockSpec(memory_space=pltpu.SMEM)] + [NEAR] * 5,
        out_specs=(FAR, NEAR),
        scratch_shapes=[
            pltpu.VMEM((rows, width // 2), jnp.bfloat16),
            pltpu.SemaphoreType.DMA((9,)),
        ],
        name="assemble",
    )(
        core.reshape(1).astype(jnp.int32), in_vmem(tokens), in_vmem(mine), in_vmem(theirs),
        in_vmem(gain), in_vmem(side),
    )


def route(line, second, rows, weights, done):
    planes, depth, _ = second.shape
    half = line.shape[1] - 256
    tiles = [
        line[:, half + 128 * k : half + 128 * (k + 1)].astype(jnp.float32) for k in range(2)
    ]
    lane = lax.broadcasted_iota(jnp.int32, (8, 128), 1)
    for which in range(3):
        for parity in range(2):
            parts = []
            for tile in tiles:
                part = jnp.zeros((8, 128), jnp.float32)
                for quarter in range(4):
                    z = 2 * quarter + parity
                    part = part + placed_lanes(
                        tile[8 * z : 8 * z + 8], lane, 32 * which, 32 * quarter, 32
                    )
                parts.append(part)
            start = 256 * which + 128 * parity
            weights[:, start : start + 128] = jnp.concatenate(parts, axis=0).astype(jnp.bfloat16)
    copies = [
        pltpu.make_async_copy(weights, second.at[k, :, pl.ds(1024, 768)], done.at[k])
        for k in range(planes)
    ]
    for copy in copies:
        copy.start()
    marks = line[:, half : half + 128]
    group = planes // 4
    count = group * depth
    for step in range(4):
        row = lax.broadcasted_iota(jnp.int32, (count, 128), 0) + step * count
        lane = lax.broadcasted_iota(jnp.int32, (count, 128), 1)
        spread = jnp.where(lane == 96 + row // depth, 1.0, 0.0).astype(jnp.bfloat16)
        place = dot(spread, marks, ((1,), (1,)))
        row, lane = row[:, : line.shape[0]], lane[:, : line.shape[0]]
        taken = (place == (1 + row % CAP).astype(jnp.float32)) & (row // CAP % 8 == lane // 8)
        taken = jnp.where(taken, 1.0, 0.0).astype(jnp.bfloat16)
        rows[pl.ds(step * group, group)] = (
            dot(taken, line[:, :half]).astype(jnp.bfloat16).reshape(group, depth, half)
        )
        copy = pltpu.make_async_copy(
            rows.at[pl.ds(step * group, group)],
            second.at[pl.ds(step * group, group), :, pl.ds(0, 1024)],
            done.at[planes + step],
        )
        copy.start()
        copies.append(copy)
    for copy in copies:
        copy.wait()


def routed_rows(line, planes):
    half = line.shape[1] - 256
    return pl.pallas_call(
        route,
        out_shape=jax.ShapeDtypeStruct((planes, 16, half + 768), jnp.bfloat16),
        in_specs=[NEAR],
        out_specs=FAR,
        scratch_shapes=[
            pltpu.VMEM((planes, 16, half), jnp.bfloat16),
            pltpu.VMEM((16, 768), jnp.bfloat16),
            pltpu.SemaphoreType.DMA((planes + 4,)),
        ],
        name="route",
    )(in_vmem(line))


def shards(
    tokens,
    first_gain,
    query_weight,
    key_weight,
    value_weight,
    decay_down,
    decay_up,
    decay_bias,
    head_gain,
    recurrent_state,
    out_weight,
    second_gain,
    expert_ids,
    route_weights,
    expert_gate,
    expert_up,
    expert_down,
    dense_gate,
    dense_up,
    dense_down,
    branch_gate,
):
    rows_dev, width = tokens.shape
    core = lax.axis_index("tp")
    lines = lax.axis_size("ep_0")
    plane = lax.axis_size(PLANE)
    half = width // 2
    rows_own, hidden = dense_gate.shape
    units = hidden // lines
    partial_value, side = attended(
        tokens, first_gain, query_weight, decay_down.T, key_weight, decay_up, decay_bias,
        value_weight, expert_ids, route_weights, dense_gate, dense_up, dense_down.T,
        recurrent_state[:, 0], head_gain, out_weight,
    )
    first, own_half = assembled(
        core, tokens, partial_value, swapped(partial_value), second_gain, side
    )
    first, gate, up, down = lax.optimization_barrier(
        (first, expert_gate[0], expert_up[0], expert_down[0])
    )
    line = exchanged(first, "ep_0")
    line = line.reshape(lines * rows_dev, half + 256)
    given = jnp.concatenate([half_of(gate, 1 - core, 0), half_of(up, 1 - core, 0)], axis=1)
    taken_in = swapped(given)
    taken_down = swapped(half_of(down, 1 - core, 1))
    inner = gate.shape[1]
    weights_in = jnp.concatenate(
        [half_of(gate, core, 0), taken_in[:, :inner], half_of(up, core, 0), taken_in[:, inner:]],
        axis=1,
    )
    weights_down = jnp.concatenate([half_of(down, core, 1), taken_down], axis=0)
    arrived = exchanged(routed_rows(line, plane), PLANE)
    slots = plane * lines * CAP
    mine = arrived[:, :, :half].reshape(slots, half)
    partial_in = jnp.dot(mine, weights_in, preferred_element_type=jnp.float32)
    blocks = [partial_in[:, k * inner : (k + 1) * inner] for k in (1, 0, 3, 2)]
    pre = partial_in + swapped(
        jnp.concatenate(blocks, axis=1).astype(jnp.bfloat16)
    ).astype(jnp.float32)
    activated = (jax.nn.silu(pre[:, : 2 * inner]) * pre[:, 2 * inner :]).astype(jnp.bfloat16)
    summed = jnp.dot(activated, weights_down, preferred_element_type=jnp.float32).astype(
        jnp.bfloat16
    )
    summed, arrived, line = lax.optimization_barrier((summed, arrived, line))
    came_back = exchanged(summed.reshape(plane, lines * CAP, half), PLANE)
    line_in = line[:, :half]
    line_rest = swapped(line_in)
    pre_gate = jnp.dot(
        line_in, half_of(branch_gate, core, 0), preferred_element_type=jnp.float32
    ) + jnp.dot(line_rest, half_of(branch_gate, 1 - core, 0), preferred_element_type=jnp.float32)
    branch = jax.nn.sigmoid(pre_gate)
    matrices = [
        jnp.concatenate(
            [
                arrived[:, :, half + 256 * m + 128 * p : half + 256 * m + 128 * (p + 1)].reshape(
                    plane * rows_own, 128
                )
                for p in range(2)
            ],
            axis=0,
        )
        for m in range(3)
    ]
    quarter = width // 4
    group = jnp.arange(128, dtype=jnp.int32)[None, :] // units
    low = jnp.where(core == 0, line_in, line_rest)
    high = jnp.where(core == 0, line_rest, line_in)

    def through(matrix):
        total = jnp.zeros((lines * rows_dev, 128), jnp.float32)
        for q in range(4):
            part = (low, high)[q // 2][:, q % 2 * quarter : (q % 2 + 1) * quarter]
            total = total + jnp.where(
                group == q, jnp.dot(part, matrix, preferred_element_type=jnp.float32), 0.0
            )
        return sum(jnp.roll(total, units * q, axis=1) for q in range(4))

    line_hidden = (jax.nn.silu(through(matrices[0])) * through(matrices[1])).astype(jnp.bfloat16)
    line_part = jnp.concatenate(
        [dot(jnp.where(group == q, line_hidden, 0), matrices[2], ((1,), (1,))) for q in range(4)],
        axis=1,
    ).astype(jnp.bfloat16)
    dense = branch[:, None] * (
        half_of(line_part, core, 1).astype(jnp.float32)
        + swapped(half_of(line_part, 1 - core, 1)).astype(jnp.float32)
    )
    row = lax.broadcasted_iota(jnp.int32, (slots, lines * rows_dev), 0)
    col = lax.broadcasted_iota(jnp.int32, (slots, lines * rows_dev), 1)
    spread = (
        lax.broadcasted_iota(jnp.int32, (slots, plane), 0) // (lines * CAP)
        == lax.broadcasted_iota(jnp.int32, (slots, plane), 1)
    ).astype(jnp.bfloat16)

    def over_slots(start):
        return dot(spread, line[:, half + start : half + start + plane], ((1,), (1,)))

    taken = (over_slots(96) == (1 + row % CAP).astype(jnp.float32)) & (
        row // CAP % lines == col // rows_dev
    )
    weighing = jnp.where(taken, over_slots(112) + over_slots(224), 0.0)
    weigh_high = weighing.astype(jnp.bfloat16)
    weigh_low = (weighing - weigh_high.astype(jnp.float32)).astype(jnp.bfloat16)

    def combined(part):
        return lax.dot_general(
            part,
            came_back.reshape(slots, half),
            (((0,), (0,)), ((), ())),
            preferred_element_type=jnp.float32,
        )

    third = (combined(weigh_high) + combined(weigh_low) + dense).astype(jnp.bfloat16)
    parts = exchanged(third.reshape(lines, rows_dev, half), "ep_0")
    return (own_half + parts.astype(jnp.float32).sum(axis=0)).astype(jnp.bfloat16)


def solution(mesh):
    split = Mesh(mesh.devices.reshape(8, 4, 4, mesh.shape["tp"]), ("ep_0", "ep_1", "ep_2", "tp"))
    placed = (
        P(EP, None),
        P(),
        P(None, "tp"),
        P(None, "tp"),
        P(None, "tp"),
        P(),
        P(None, "tp"),
        P("tp"),
        P(),
        P(EP, "tp", None, None),
        P("tp", None),
        P(),
        P(EP, None),
        P(EP, None),
        P(EP, None, "tp"),
        P(EP, None, "tp"),
        P(EP, "tp", None),
        P(EP, "tp"),
        P(EP, "tp"),
        P("tp", EP),
        P(),
    )
    return jax.shard_map(
        shards, mesh=split, in_specs=placed, out_specs=P(EP, "tp"), check_vma=False
    )
```

```python
import jax
import jax.numpy as jnp
from jax import lax
from jax.sharding import Mesh
from jax.sharding import PartitionSpec as P

from jax.experimental import pallas as pl
from jax.experimental.pallas import tpu as pltpu

DK = 128
TOPK = 6
EP = ("ep_0", "ep_1", "ep_2")
PLANE = ("ep_1", "ep_2")
CAP = 2


EPS = 1e-06


SWAP = [(0, 1), (1, 0)]


def swapped(array):
    return lax.ppermute(array, "tp", SWAP)


def half_of(array, index, dim):
    width = array.shape[dim] // 2
    return lax.dynamic_slice_in_dim(array, index * width, width, dim)


def exchanged(array, axis):
    return lax.all_to_all(array, axis, split_axis=0, concat_axis=0, tiled=True)


def rms_scale(values_in, gain):
    widened = values_in.astype(jnp.float32)
    return (
        widened
        * lax.rsqrt(jnp.mean(widened * widened, axis=-1, keepdims=True) + EPS)
        * gain.astype(jnp.float32)
    )


def dot(a, b, dims=((1,), (0,))):
    return lax.dot_general(a, b, (dims, ((), ())), preferred_element_type=jnp.float32)


FAR = pl.BlockSpec(memory_space=pl.ANY)
NEAR = pl.BlockSpec(memory_space=pltpu.VMEM)
SMALL = pltpu.CompilerParams(vmem_limit_bytes=32 * 2**20)


def in_vmem(array):
    return pltpu.with_memory_space_constraint(array, pltpu.VMEM)


def placed_lanes(tile, lane, source, target, size):
    shift = (target - source) % 128
    turned = tile if shift == 0 else pltpu.roll(tile, shift, 1)
    return jnp.where((lane >= target) & (lane < target + size), turned, 0.0)


def attend(*refs):
    far, result, side, near, done = refs[:16], refs[16], refs[17], refs[18:34], refs[34]
    copies = [pltpu.make_async_copy(far[k], near[k], done.at[k]) for k in range(16)]
    for copy in copies:
        copy.start()
    (
        tokens, gain, query_weight, decay_down, key_weight, decay_up, decay_bias, value_weight,
        ids, weights, dense_gate, dense_up, dense_down, state, head_gain, out_weight,
    ) = near
    count = tokens.shape[0]
    copies[0].wait()
    copies[1].wait()
    normed = rms_scale(tokens[...], gain[...][None, :]).astype(jnp.bfloat16)
    copies[2].wait()
    query = dot(normed, query_weight[...]) * DK ** (-0.5)
    copies[3].wait()
    decay_low = dot(normed, decay_down[...], ((1,), (1,))).astype(jnp.bfloat16)
    copies[4].wait()
    keys = dot(normed, key_weight[...])
    copies[5].wait()
    copies[6].wait()
    decay_pre = dot(decay_low, decay_up[...]) + decay_bias[...][None, :]
    log_decay = jnp.minimum(decay_pre, 0.0) - jnp.log1p(jnp.exp(-jnp.abs(decay_pre)))
    columns = jnp.transpose(query * jnp.exp(log_decay / 16.0))
    copies[7].wait()
    values = dot(normed, value_weight[...])

    for k in range(8, 13):
        copies[k].wait()
    lane = lax.broadcasted_iota(jnp.int32, (8, 128), 1)
    line = lax.broadcasted_iota(jnp.int32, (8, 128), 0)
    shares = weights[...] / jnp.sum(weights[...], axis=1, keepdims=True)
    chosen = jnp.zeros((8, 128), jnp.float32)
    share = jnp.zeros((8, 128), jnp.float32)
    for k in range(TOPK):
        named = ids[:, k : k + 1] == lane
        chosen = chosen + jnp.where(named, 1.0, 0.0)
        share = share + jnp.where(named, shares[:, k : k + 1], 0.0)
    place = jnp.where(chosen > 0.0, 1.0, 0.0)
    for k in range(1, count):
        place = place + jnp.where(line >= k, pltpu.roll(chosen, k, 0), 0.0)
    place = place * chosen
    share_high = share.astype(jnp.bfloat16).astype(jnp.float32)
    share_low = share - share_high
    for z in range(8):
        tiles = []
        for part in range(2):
            tile = jnp.zeros((8, 128), jnp.float32)
            for m, matrix in enumerate((dense_gate, dense_up, dense_down)):
                start = 128 * (z // 4)
                piece = matrix[...].astype(jnp.float32)[8 * part : 8 * part + 8, start : start + 128]
                tile = tile + placed_lanes(piece, lane, 32 * (z % 4), 32 * m, 32)
            tiles.append(tile)
        tiles[0] = tiles[0] + placed_lanes(place, lane, 16 * z, 96, 16)
        tiles[0] = tiles[0] + placed_lanes(share_high, lane, 16 * z, 112, 16)
        tiles[1] = tiles[1] + placed_lanes(share_low, lane, 16 * z, 96, 16)
        side[z] = jnp.concatenate(tiles, axis=1).astype(jnp.bfloat16)

    copies[13].wait()
    read = [
        jnp.sum(columns[:, k : k + 1] * state[k], axis=0, keepdims=True) for k in range(count)
    ]
    head = jnp.concatenate(read, axis=0) + jnp.sum(query * keys, axis=1, keepdims=True) * values
    copies[14].wait()
    head = rms_scale(head, head_gain[...][None, :]).astype(jnp.bfloat16)
    copies[15].wait()
    result[...] = dot(head, out_weight[...]).astype(jnp.bfloat16)


def attended(*held):
    tokens = held[0]
    return pl.pallas_call(
        attend,
        out_shape=(
            pltpu.VMEM(tokens.shape, jnp.bfloat16),
            pltpu.VMEM((8, 8, 256), jnp.bfloat16),
        ),
        in_specs=[FAR] * 16,
        out_specs=(NEAR, NEAR),
        scratch_shapes=[pltpu.VMEM(a.shape, a.dtype) for a in held]
        + [pltpu.SemaphoreType.DMA((16,))],
        name="attend",
    )(*held)


def assemble(core, tokens, mine, theirs, gain, side, first, own, block, done):
    sides = pltpu.make_async_copy(side, first.at[:, :, pl.ds(1024, 256)], done.at[8])
    sides.start()
    both = mine[...].astype(jnp.float32) + theirs[...].astype(jnp.float32)
    residual = (tokens[...].astype(jnp.float32) + both).astype(jnp.bfloat16)
    normed = rms_scale(residual, gain[...][None, :])
    half = normed.shape[1] // 2
    first_half = core[0] == 0
    block[...] = jnp.where(first_half, normed[:, :half], normed[:, half:]).astype(jnp.bfloat16)
    copies = [
        pltpu.make_async_copy(block, first.at[z, :, pl.ds(0, 1024)], done.at[z]) for z in range(8)
    ]
    for copy in copies:
        copy.start()
    wide = residual.astype(jnp.float32)
    own[...] = jnp.where(first_half, wide[:, :half], wide[:, half:])
    for copy in copies:
        copy.wait()
    sides.wait()


def assembled(core, tokens, mine, theirs, gain, side):
    rows, width = tokens.shape
    return pl.pallas_call(
        assemble,
        out_shape=(
            jax.ShapeDtypeStruct((8, rows, width // 2 + 256), jnp.bfloat16),
            pltpu.VMEM((rows, width // 2), jnp.float32),
        ),
        in_specs=[pl.BlockSpec(memory_space=pltpu.SMEM)] + [NEAR] * 5,
        out_specs=(FAR, NEAR),
        scratch_shapes=[
            pltpu.VMEM((rows, width // 2), jnp.bfloat16),
            pltpu.SemaphoreType.DMA((9,)),
        ],
        compiler_params=SMALL,
        name="assemble",
    )(
        core, in_vmem(tokens), in_vmem(mine), in_vmem(theirs),
        in_vmem(gain), in_vmem(side),
    )


def route(line, second, weights):
    planes, depth, _ = second.shape
    half = line.shape[1] - 256
    tiles = [
        line[:, half + 128 * k : half + 128 * (k + 1)].astype(jnp.float32) for k in range(2)
    ]
    lane = lax.broadcasted_iota(jnp.int32, (8, 128), 1)
    for which in range(3):
        for parity in range(2):
            parts = []
            for tile in tiles:
                part = jnp.zeros((8, 128), jnp.float32)
                for quarter in range(4):
                    z = 2 * quarter + parity
                    part = part + placed_lanes(
                        tile[8 * z : 8 * z + 8], lane, 32 * which, 32 * quarter, 32
                    )
                parts.append(part)
            start = 256 * which + 128 * parity
            weights[:, start : start + 128] = jnp.concatenate(parts, axis=0).astype(jnp.bfloat16)
    second[:, :, half:] = jnp.broadcast_to(weights[...][None], (planes, depth, 768))
    marks = line[:, half : half + 128]
    count = planes * depth
    row = lax.broadcasted_iota(jnp.int32, (count, 128), 0)
    lane = lax.broadcasted_iota(jnp.int32, (count, 128), 1)
    spread = jnp.where(lane == 96 + row // depth, 1.0, 0.0).astype(jnp.bfloat16)
    place = dot(spread, marks, ((1,), (1,)))
    row, lane = row[:, : line.shape[0]], lane[:, : line.shape[0]]
    taken = (place == (1 + row % CAP).astype(jnp.float32)) & (row // CAP % 8 == lane // 8)
    taken = jnp.where(taken, 1.0, 0.0).astype(jnp.bfloat16)
    second[:, :, :half] = (
        dot(taken, line[:, :half]).astype(jnp.bfloat16).reshape(planes, depth, half)
    )


def routed_rows(line, planes):
    half = line.shape[1] - 256
    return pl.pallas_call(
        route,
        out_shape=pltpu.VMEM((planes, 16, half + 768), jnp.bfloat16),
        in_specs=[NEAR],
        out_specs=NEAR,
        scratch_shapes=[pltpu.VMEM((16, 768), jnp.bfloat16)],
        compiler_params=SMALL,
        name="route",
    )(in_vmem(line))


def widen(core, arrived, gate, up, far, pre, sent):
    planes, depth, _ = arrived.shape
    half, wide = far.shape
    units = wide // 2
    rows = arrived[:, :, :half].reshape(planes * depth, half)
    start = pl.multiple_of(core[0] * half, half)
    there = dot(rows, far[...])
    here = [dot(rows, matrix[pl.ds(start, half), :]) for matrix in (gate, up)]
    parts = (here[0], there[:, :units], here[1], there[:, units:])
    for k in range(4):
        pre[:, k * units : (k + 1) * units] = parts[k]
        sent[:, k * units : (k + 1) * units] = parts[k ^ 1].astype(jnp.bfloat16)


def widened(core, arrived, gate, up, far):
    slots, wide = arrived.shape[0] * arrived.shape[1], 2 * far.shape[1]
    return pl.pallas_call(
        widen,
        out_shape=(
            pltpu.VMEM((slots, wide), jnp.float32),
            pltpu.VMEM((slots, wide), jnp.bfloat16),
        ),
        in_specs=[pl.BlockSpec(memory_space=pltpu.SMEM)] + [NEAR] * 4,
        out_specs=(NEAR, NEAR),
        compiler_params=SMALL,
        name="widen",
    )(core, *[in_vmem(a) for a in (arrived, gate, up, far)])


def narrow(core, pre, came, down, far, result, rows, done):
    units = far.shape[0]
    planes, depth, half = result.shape
    start = pl.multiple_of(core[0] * half, half)
    near = down[:, pl.ds(start, half)]
    group = planes // 4
    count = group * depth
    copies = []
    for step in range(4):
        part = slice(step * count, (step + 1) * count)
        total = pre[part, :] + came[part, :].astype(jnp.float32)
        gate = total[:, : 2 * units]
        hidden = (gate / (1.0 + jnp.exp(-gate)) * total[:, 2 * units :]).astype(jnp.bfloat16)
        out = dot(hidden[:, :units], near) + dot(hidden[:, units:], far[...])
        here = pl.ds(step * group, group)
        rows[here] = out.astype(jnp.bfloat16).reshape(group, depth, half)
        copy = pltpu.make_async_copy(rows.at[here], result.at[here], done.at[step])
        copy.start()
        copies.append(copy)
    for copy in copies:
        copy.wait()


def narrowed(core, pre, came, down, far, planes):
    shape = (planes, pre.shape[0] // planes, far.shape[1])
    return pl.pallas_call(
        narrow,
        out_shape=jax.ShapeDtypeStruct(shape, jnp.bfloat16),
        in_specs=[pl.BlockSpec(memory_space=pltpu.SMEM)] + [NEAR] * 4,
        out_specs=FAR,
        scratch_shapes=[pltpu.VMEM(shape, jnp.bfloat16), pltpu.SemaphoreType.DMA((4,))],
        compiler_params=SMALL,
        name="narrow",
    )(core, *[in_vmem(a) for a in (pre, came, down, far)])


def shards(
    tokens,
    first_gain,
    query_weight,
    key_weight,
    value_weight,
    decay_down,
    decay_up,
    decay_bias,
    head_gain,
    recurrent_state,
    out_weight,
    second_gain,
    expert_ids,
    route_weights,
    expert_gate,
    expert_up,
    expert_down,
    dense_gate,
    dense_up,
    dense_down,
    branch_gate,
):
    rows_dev, width = tokens.shape
    core = lax.axis_index("tp")
    lines = lax.axis_size("ep_0")
    plane = lax.axis_size(PLANE)
    half = width // 2
    rows_own, hidden = dense_gate.shape
    units = hidden // lines
    partial_value, side = attended(
        tokens, first_gain, query_weight, decay_down.T, key_weight, decay_up, decay_bias,
        value_weight, expert_ids, route_weights, dense_gate, dense_up, dense_down.T,
        recurrent_state[:, 0], head_gain, out_weight,
    )
    which = core.reshape(1).astype(jnp.int32)
    first, own_half = assembled(
        which, tokens, partial_value, swapped(partial_value), second_gain, side
    )
    first, gate, up, down = lax.optimization_barrier(
        (first, expert_gate[0], expert_up[0], expert_down[0])
    )
    line = exchanged(first, "ep_0")
    line = line.reshape(lines * rows_dev, half + 256)
    given = jnp.concatenate([half_of(gate, 1 - core, 0), half_of(up, 1 - core, 0)], axis=1)
    far_in = swapped(given)
    far_down = swapped(half_of(down, 1 - core, 1))
    line, far_in, far_down, gate, up, down = lax.optimization_barrier(
        (line, far_in, far_down, gate, up, down)
    )
    arrived = exchanged(routed_rows(line, plane), PLANE)
    slots = plane * lines * CAP
    pre, sent = widened(which, arrived, gate, up, far_in)
    summed = narrowed(which, pre, swapped(sent), down, far_down, plane)
    summed, arrived, line = lax.optimization_barrier((summed, arrived, line))
    came_back = exchanged(summed, PLANE)
    line_in = line[:, :half]
    line_rest = swapped(line_in)
    pre_gate = jnp.dot(
        line_in, half_of(branch_gate, core, 0), preferred_element_type=jnp.float32
    ) + jnp.dot(line_rest, half_of(branch_gate, 1 - core, 0), preferred_element_type=jnp.float32)
    branch = jax.nn.sigmoid(pre_gate)
    matrices = [
        jnp.concatenate(
            [
                arrived[:, :, half + 256 * m + 128 * p : half + 256 * m + 128 * (p + 1)].reshape(
                    plane * rows_own, 128
                )
                for p in range(2)
            ],
            axis=0,
        )
        for m in range(3)
    ]
    quarter = width // 4
    group = jnp.arange(128, dtype=jnp.int32)[None, :] // units
    low = jnp.where(core == 0, line_in, line_rest)
    high = jnp.where(core == 0, line_rest, line_in)

    def through(matrix):
        total = jnp.zeros((lines * rows_dev, 128), jnp.float32)
        for q in range(4):
            part = (low, high)[q // 2][:, q % 2 * quarter : (q % 2 + 1) * quarter]
            total = total + jnp.where(
                group == q, jnp.dot(part, matrix, preferred_element_type=jnp.float32), 0.0
            )
        return sum(jnp.roll(total, units * q, axis=1) for q in range(4))

    line_hidden = (jax.nn.silu(through(matrices[0])) * through(matrices[1])).astype(jnp.bfloat16)
    line_part = jnp.concatenate(
        [dot(jnp.where(group == q, line_hidden, 0), matrices[2], ((1,), (1,))) for q in range(4)],
        axis=1,
    ).astype(jnp.bfloat16)
    dense = branch[:, None] * (
        half_of(line_part, core, 1).astype(jnp.float32)
        + swapped(half_of(line_part, 1 - core, 1)).astype(jnp.float32)
    )
    row = lax.broadcasted_iota(jnp.int32, (slots, lines * rows_dev), 0)
    col = lax.broadcasted_iota(jnp.int32, (slots, lines * rows_dev), 1)
    spread = (
        lax.broadcasted_iota(jnp.int32, (slots, plane), 0) // (lines * CAP)
        == lax.broadcasted_iota(jnp.int32, (slots, plane), 1)
    ).astype(jnp.bfloat16)

    def over_slots(start):
        return dot(spread, line[:, half + start : half + start + plane], ((1,), (1,)))

    taken = (over_slots(96) == (1 + row % CAP).astype(jnp.float32)) & (
        row // CAP % lines == col // rows_dev
    )
    weighing = jnp.where(taken, over_slots(112) + over_slots(224), 0.0)
    weigh_high = weighing.astype(jnp.bfloat16)
    weigh_low = (weighing - weigh_high.astype(jnp.float32)).astype(jnp.bfloat16)

    def combined(part):
        return lax.dot_general(
            part,
            came_back.reshape(slots, half),
            (((0,), (0,)), ((), ())),
            preferred_element_type=jnp.float32,
        )

    third = (combined(weigh_high) + combined(weigh_low) + dense).astype(jnp.bfloat16)
    parts = exchanged(third.reshape(lines, rows_dev, half), "ep_0")
    return (own_half + parts.astype(jnp.float32).sum(axis=0)).astype(jnp.bfloat16)


def solution(mesh):
    split = Mesh(mesh.devices.reshape(8, 4, 4, mesh.shape["tp"]), ("ep_0", "ep_1", "ep_2", "tp"))
    placed = (
        P(EP, None),
        P(),
        P(None, "tp"),
        P(None, "tp"),
        P(None, "tp"),
        P(),
        P(None, "tp"),
        P("tp"),
        P(),
        P(EP, "tp", None, None),
        P("tp", None),
        P(),
        P(EP, None),
        P(EP, None),
        P(EP, None, "tp"),
        P(EP, None, "tp"),
        P(EP, "tp", None),
        P(EP, "tp"),
        P(EP, "tp"),
        P("tp", EP),
        P(),
    )
    return jax.shard_map(
        shards, mesh=split, in_specs=placed, out_specs=P(EP, "tp"), check_vma=False
    )
```

```python
import jax
import jax.numpy as jnp
from jax import lax
from jax.sharding import Mesh
from jax.sharding import PartitionSpec as P

from jax.experimental import pallas as pl
from jax.experimental.pallas import tpu as pltpu

DK = 128
TOPK = 6
EP = ("ep_0", "ep_1", "ep_2")
PLANE = ("ep_1", "ep_2")
CAP = 2


EPS = 1e-06


SWAP = [(0, 1), (1, 0)]


def swapped(array):
    return lax.ppermute(array, "tp", SWAP)


def half_of(array, index, dim):
    width = array.shape[dim] // 2
    return lax.dynamic_slice_in_dim(array, index * width, width, dim)


def exchanged(array, axis):
    return lax.all_to_all(array, axis, split_axis=0, concat_axis=0, tiled=True)


def rms_scale(values_in, gain):
    widened = values_in.astype(jnp.float32)
    return (
        widened
        * lax.rsqrt(jnp.mean(widened * widened, axis=-1, keepdims=True) + EPS)
        * gain.astype(jnp.float32)
    )


def dot(a, b, dims=((1,), (0,))):
    return lax.dot_general(a, b, (dims, ((), ())), preferred_element_type=jnp.float32)


FAR = pl.BlockSpec(memory_space=pl.ANY)
NEAR = pl.BlockSpec(memory_space=pltpu.VMEM)
SMALL = pltpu.CompilerParams(vmem_limit_bytes=32 * 2**20)


def in_vmem(array):
    return pltpu.with_memory_space_constraint(array, pltpu.VMEM)


def placed_lanes(tile, lane, source, target, size):
    shift = (target - source) % 128
    turned = tile if shift == 0 else pltpu.roll(tile, shift, 1)
    return jnp.where((lane >= target) & (lane < target + size), turned, 0.0)


def attend(*refs):
    far, result, side, near, done = refs[:16], refs[16], refs[17], refs[18:34], refs[34]
    copies = [pltpu.make_async_copy(far[k], near[k], done.at[k]) for k in range(16)]
    for copy in copies:
        copy.start()
    (
        tokens, gain, query_weight, decay_down, key_weight, decay_up, decay_bias, value_weight,
        ids, weights, dense_gate, dense_up, dense_down, state, head_gain, out_weight,
    ) = near
    count = tokens.shape[0]
    copies[0].wait()
    copies[1].wait()
    normed = rms_scale(tokens[...], gain[...][None, :]).astype(jnp.bfloat16)
    copies[2].wait()
    query = dot(normed, query_weight[...]) * DK ** (-0.5)
    copies[3].wait()
    decay_low = dot(normed, decay_down[...], ((1,), (1,))).astype(jnp.bfloat16)
    copies[4].wait()
    keys = dot(normed, key_weight[...])
    copies[5].wait()
    copies[6].wait()
    decay_pre = dot(decay_low, decay_up[...]) + decay_bias[...][None, :]
    log_decay = jnp.minimum(decay_pre, 0.0) - jnp.log1p(jnp.exp(-jnp.abs(decay_pre)))
    columns = jnp.transpose(query * jnp.exp(log_decay / 16.0))
    copies[7].wait()
    values = dot(normed, value_weight[...])

    for k in range(8, 13):
        copies[k].wait()
    lane = lax.broadcasted_iota(jnp.int32, (8, 128), 1)
    line = lax.broadcasted_iota(jnp.int32, (8, 128), 0)
    shares = weights[...] / jnp.sum(weights[...], axis=1, keepdims=True)
    chosen = jnp.zeros((8, 128), jnp.float32)
    share = jnp.zeros((8, 128), jnp.float32)
    for k in range(TOPK):
        named = ids[:, k : k + 1] == lane
        chosen = chosen + jnp.where(named, 1.0, 0.0)
        share = share + jnp.where(named, shares[:, k : k + 1], 0.0)
    place = jnp.where(chosen > 0.0, 1.0, 0.0)
    for k in range(1, count):
        place = place + jnp.where(line >= k, pltpu.roll(chosen, k, 0), 0.0)
    place = place * chosen
    share_high = share.astype(jnp.bfloat16).astype(jnp.float32)
    share_low = share - share_high
    for z in range(8):
        tiles = []
        for part in range(2):
            tile = jnp.zeros((8, 128), jnp.float32)
            for m, matrix in enumerate((dense_gate, dense_up, dense_down)):
                start = 128 * (z // 4)
                piece = matrix[...].astype(jnp.float32)[8 * part : 8 * part + 8, start : start + 128]
                tile = tile + placed_lanes(piece, lane, 32 * (z % 4), 32 * m, 32)
            tiles.append(tile)
        tiles[0] = tiles[0] + placed_lanes(place, lane, 16 * z, 96, 16)
        tiles[0] = tiles[0] + placed_lanes(share_high, lane, 16 * z, 112, 16)
        tiles[1] = tiles[1] + placed_lanes(share_low, lane, 16 * z, 96, 16)
        side[z] = jnp.concatenate(tiles, axis=1).astype(jnp.bfloat16)

    copies[13].wait()
    read = [
        jnp.sum(columns[:, k : k + 1] * state[k], axis=0, keepdims=True) for k in range(count)
    ]
    head = jnp.concatenate(read, axis=0) + jnp.sum(query * keys, axis=1, keepdims=True) * values
    copies[14].wait()
    head = rms_scale(head, head_gain[...][None, :]).astype(jnp.bfloat16)
    copies[15].wait()
    result[...] = dot(head, out_weight[...]).astype(jnp.bfloat16)


def attended(*held):
    tokens = held[0]
    return pl.pallas_call(
        attend,
        out_shape=(
            pltpu.VMEM(tokens.shape, jnp.bfloat16),
            pltpu.VMEM((8, 8, 256), jnp.bfloat16),
        ),
        in_specs=[FAR] * 16,
        out_specs=(NEAR, NEAR),
        scratch_shapes=[pltpu.VMEM(a.shape, a.dtype) for a in held]
        + [pltpu.SemaphoreType.DMA((16,))],
        name="attend",
    )(*held)


def assemble(core, tokens, mine, theirs, gain, side, first, own, block, done):
    sides = pltpu.make_async_copy(side, first.at[:, :, pl.ds(1024, 256)], done.at[8])
    sides.start()
    both = mine[...].astype(jnp.float32) + theirs[...].astype(jnp.float32)
    residual = (tokens[...].astype(jnp.float32) + both).astype(jnp.bfloat16)
    normed = rms_scale(residual, gain[...][None, :])
    half = normed.shape[1] // 2
    first_half = core[0] == 0
    block[...] = jnp.where(first_half, normed[:, :half], normed[:, half:]).astype(jnp.bfloat16)
    copies = [
        pltpu.make_async_copy(block, first.at[z, :, pl.ds(0, 1024)], done.at[z]) for z in range(8)
    ]
    for copy in copies:
        copy.start()
    wide = residual.astype(jnp.float32)
    own[...] = jnp.where(first_half, wide[:, :half], wide[:, half:])
    for copy in copies:
        copy.wait()
    sides.wait()


def assembled(core, tokens, mine, theirs, gain, side):
    rows, width = tokens.shape
    return pl.pallas_call(
        assemble,
        out_shape=(
            jax.ShapeDtypeStruct((8, rows, width // 2 + 256), jnp.bfloat16),
            pltpu.VMEM((rows, width // 2), jnp.float32),
        ),
        in_specs=[pl.BlockSpec(memory_space=pltpu.SMEM)] + [NEAR] * 5,
        out_specs=(FAR, NEAR),
        scratch_shapes=[
            pltpu.VMEM((rows, width // 2), jnp.bfloat16),
            pltpu.SemaphoreType.DMA((9,)),
        ],
        compiler_params=SMALL,
        name="assemble",
    )(
        core, in_vmem(tokens), in_vmem(mine), in_vmem(theirs),
        in_vmem(gain), in_vmem(side),
    )


def route(line, second, copy, weights):
    planes, depth, _ = second.shape
    half = line.shape[1] - 256
    tiles = [
        line[:, half + 128 * k : half + 128 * (k + 1)].astype(jnp.float32) for k in range(2)
    ]
    lane = lax.broadcasted_iota(jnp.int32, (8, 128), 1)
    for which in range(3):
        for parity in range(2):
            parts = []
            for tile in tiles:
                part = jnp.zeros((8, 128), jnp.float32)
                for quarter in range(4):
                    z = 2 * quarter + parity
                    part = part + placed_lanes(
                        tile[8 * z : 8 * z + 8], lane, 32 * which, 32 * quarter, 32
                    )
                parts.append(part)
            start = 256 * which + 128 * parity
            weights[:, start : start + 128] = jnp.concatenate(parts, axis=0).astype(jnp.bfloat16)
    second[:, :, half:] = jnp.broadcast_to(weights[...][None], (planes, depth, 768))
    copy[...] = line[:, :half]
    marks = line[:, half : half + 128]
    count = planes * depth
    row = lax.broadcasted_iota(jnp.int32, (count, 128), 0)
    lane = lax.broadcasted_iota(jnp.int32, (count, 128), 1)
    spread = jnp.where(lane == 96 + row // depth, 1.0, 0.0).astype(jnp.bfloat16)
    place = dot(spread, marks, ((1,), (1,)))
    row, lane = row[:, : line.shape[0]], lane[:, : line.shape[0]]
    taken = (place == (1 + row % CAP).astype(jnp.float32)) & (row // CAP % 8 == lane // 8)
    taken = jnp.where(taken, 1.0, 0.0).astype(jnp.bfloat16)
    second[:, :, :half] = (
        dot(taken, line[:, :half]).astype(jnp.bfloat16).reshape(planes, depth, half)
    )


def routed_rows(line, planes):
    half = line.shape[1] - 256
    return pl.pallas_call(
        route,
        out_shape=(
            pltpu.VMEM((planes, 16, half + 768), jnp.bfloat16),
            pltpu.VMEM((line.shape[0], half), jnp.bfloat16),
        ),
        in_specs=[NEAR],
        out_specs=(NEAR, NEAR),
        scratch_shapes=[pltpu.VMEM((16, 768), jnp.bfloat16)],
        compiler_params=SMALL,
        name="route",
    )(in_vmem(line))


def widen(core, arrived, gate, up, far, pre, sent):
    planes, depth, _ = arrived.shape
    half, wide = far.shape
    units = wide // 2
    rows = arrived[:, :, :half].reshape(planes * depth, half)
    start = pl.multiple_of(core[0] * half, half)
    there = dot(rows, far[...])
    here = [dot(rows, matrix[pl.ds(start, half), :]) for matrix in (gate, up)]
    parts = (here[0], there[:, :units], here[1], there[:, units:])
    for k in range(4):
        pre[:, k * units : (k + 1) * units] = parts[k]
        sent[:, k * units : (k + 1) * units] = parts[k ^ 1].astype(jnp.bfloat16)


def widened(core, arrived, gate, up, far):
    slots, wide = arrived.shape[0] * arrived.shape[1], 2 * far.shape[1]
    return pl.pallas_call(
        widen,
        out_shape=(
            pltpu.VMEM((slots, wide), jnp.float32),
            pltpu.VMEM((slots, wide), jnp.bfloat16),
        ),
        in_specs=[pl.BlockSpec(memory_space=pltpu.SMEM)] + [NEAR] * 4,
        out_specs=(NEAR, NEAR),
        compiler_params=SMALL,
        name="widen",
    )(core, *[in_vmem(a) for a in (arrived, gate, up, far)])


def narrow(core, pre, came, down, far, result):
    units = far.shape[0]
    planes, depth, half = result.shape
    start = pl.multiple_of(core[0] * half, half)
    near = down[:, pl.ds(start, half)]
    total = pre[...] + came[...].astype(jnp.float32)
    gate = total[:, : 2 * units]
    hidden = (gate / (1.0 + jnp.exp(-gate)) * total[:, 2 * units :]).astype(jnp.bfloat16)
    out = dot(hidden[:, :units], near) + dot(hidden[:, units:], far[...])
    result[...] = out.astype(jnp.bfloat16).reshape(planes, depth, half)


def narrowed(core, pre, came, down, far, planes):
    shape = (planes, pre.shape[0] // planes, far.shape[1])
    return pl.pallas_call(
        narrow,
        out_shape=pltpu.VMEM(shape, jnp.bfloat16),
        in_specs=[pl.BlockSpec(memory_space=pltpu.SMEM)] + [NEAR] * 4,
        out_specs=NEAR,
        compiler_params=SMALL,
        name="narrow",
    )(core, *[in_vmem(a) for a in (pre, came, down, far)])


def branch_out(core, arrived, line, rest, mark_own, mark_rest, keep, sent, high, low):
    planes, depth, _ = arrived.shape
    count, half = rest.shape
    quarter = half // 2

    def matrix(m):
        starts = [half + 256 * m + 128 * p for p in range(2)]
        blocks = [arrived[:, :, at : at + 128].reshape(planes * depth, 128) for at in starts]
        return jnp.concatenate(blocks, axis=0)

    group = lax.broadcasted_iota(jnp.int32, (count, 128), 1) // 32
    both = jnp.concatenate([matrix(0), matrix(1)], axis=1)
    gate = jnp.zeros((count, 128), jnp.float32)
    up = jnp.zeros((count, 128), jnp.float32)
    pre = jnp.zeros((count, 1), jnp.float32)
    for source, marks, first in (
        (line[:, :half], mark_own, 2 * core[0]),
        (rest[...], mark_rest, 2 - 2 * core[0]),
    ):
        wide = source.astype(jnp.float32) * marks[...].astype(jnp.float32)[None, :]
        pre = pre + jnp.sum(wide, axis=1, keepdims=True)
        for k in range(2):
            part = dot(source[:, k * quarter : (k + 1) * quarter], both)
            gate = gate + jnp.where(group == first + k, part[:, :128], 0.0)
            up = up + jnp.where(group == first + k, part[:, 128:], 0.0)

    def folded(total):
        return total + sum(pltpu.roll(total, 32 * k, 1) for k in range(1, 4))

    gate = folded(gate)
    hidden = gate / (1.0 + jnp.exp(-gate)) * folded(up)
    branch = 1.0 / (1.0 + jnp.exp(-pre))
    down = matrix(2)
    for target, first in ((sent, 2 - 2 * core[0]), (keep, 2 * core[0])):
        for k in range(2):
            units = jnp.where(group == first + k, hidden, 0.0).astype(jnp.bfloat16)
            target[:, k * quarter : (k + 1) * quarter] = (
                branch * dot(units, down, ((1,), (1,)))
            ).astype(jnp.bfloat16)

    slots = planes * depth
    row = lax.broadcasted_iota(jnp.int32, (slots, 128), 0)
    lane = lax.broadcasted_iota(jnp.int32, (slots, 128), 1)

    def over_slots(start, tile):
        spread = jnp.where(lane == start + row // depth, 1.0, 0.0).astype(jnp.bfloat16)
        return dot(spread, line[:, half + 128 * tile : half + 128 * (tile + 1)], ((1,), (1,)))

    place, share = over_slots(96, 0), over_slots(112, 0) + over_slots(96, 1)
    row, lane = row[:, :count], lane[:, :count]
    taken = (place == (1 + row % CAP).astype(jnp.float32)) & (row // CAP % 8 == lane // 8)
    weighing = jnp.where(taken, share, 0.0)
    upper = weighing.astype(jnp.bfloat16)
    high[...] = upper
    low[...] = (weighing - upper.astype(jnp.float32)).astype(jnp.bfloat16)


def branched_out(core, arrived, line, rest, mark_own, mark_rest):
    slots = arrived.shape[0] * arrived.shape[1]
    return pl.pallas_call(
        branch_out,
        out_shape=tuple(
            pltpu.VMEM(shape, jnp.bfloat16)
            for shape in (rest.shape, rest.shape, (slots, line.shape[0]), (slots, line.shape[0]))
        ),
        in_specs=[pl.BlockSpec(memory_space=pltpu.SMEM)] + [NEAR] * 5,
        out_specs=(NEAR,) * 4,
        compiler_params=SMALL,
        name="branch_out",
    )(core, *[in_vmem(a) for a in (arrived, line, rest, mark_own, mark_rest)])


def shards(
    tokens,
    first_gain,
    query_weight,
    key_weight,
    value_weight,
    decay_down,
    decay_up,
    decay_bias,
    head_gain,
    recurrent_state,
    out_weight,
    second_gain,
    expert_ids,
    route_weights,
    expert_gate,
    expert_up,
    expert_down,
    dense_gate,
    dense_up,
    dense_down,
    branch_gate,
):
    rows_dev, width = tokens.shape
    core = lax.axis_index("tp")
    lines = lax.axis_size("ep_0")
    plane = lax.axis_size(PLANE)
    half = width // 2
    partial_value, side = attended(
        tokens, first_gain, query_weight, decay_down.T, key_weight, decay_up, decay_bias,
        value_weight, expert_ids, route_weights, dense_gate, dense_up, dense_down.T,
        recurrent_state[:, 0], head_gain, out_weight,
    )
    which = core.reshape(1).astype(jnp.int32)
    first, own_half = assembled(
        which, tokens, partial_value, swapped(partial_value), second_gain, side
    )
    first, gate, up, down = lax.optimization_barrier(
        (first, expert_gate[0], expert_up[0], expert_down[0])
    )
    line = exchanged(first, "ep_0")
    line = line.reshape(lines * rows_dev, half + 256)
    given = jnp.concatenate([half_of(gate, 1 - core, 0), half_of(up, 1 - core, 0)], axis=1)
    far_in = swapped(given)
    mark_own = half_of(branch_gate, core, 0)
    mark_rest = half_of(branch_gate, 1 - core, 0)
    far_down = swapped(half_of(down, 1 - core, 1))
    line, far_in, far_down, gate, up, down, mark_own, mark_rest = lax.optimization_barrier(
        (line, far_in, far_down, gate, up, down, mark_own, mark_rest)
    )
    second, line_half = routed_rows(line, plane)
    arrived = exchanged(second, PLANE)
    arrived, line_half = lax.optimization_barrier((arrived, line_half))
    slots = plane * lines * CAP
    rest = swapped(line_half)
    pre, sent = widened(which, arrived, gate, up, far_in)
    came = swapped(sent)
    keep, given_part, weigh_high, weigh_low = branched_out(
        which, arrived, line, rest, mark_own, mark_rest
    )
    given_part = swapped(given_part)
    summed = narrowed(which, pre, came, down, far_down, plane)
    dense = keep.astype(jnp.float32) + given_part.astype(jnp.float32)
    summed, dense, weigh_high, weigh_low = lax.optimization_barrier(
        (summed, dense, weigh_high, weigh_low)
    )
    came_back = exchanged(summed, PLANE)

    def combined(part):
        return lax.dot_general(
            part,
            came_back.reshape(slots, half),
            (((0,), (0,)), ((), ())),
            preferred_element_type=jnp.float32,
        )

    third = (combined(weigh_high) + combined(weigh_low) + dense).astype(jnp.bfloat16)
    parts = exchanged(third.reshape(lines, rows_dev, half), "ep_0")
    return (own_half + parts.astype(jnp.float32).sum(axis=0)).astype(jnp.bfloat16)


def solution(mesh):
    split = Mesh(mesh.devices.reshape(8, 4, 4, mesh.shape["tp"]), ("ep_0", "ep_1", "ep_2", "tp"))
    placed = (
        P(EP, None),
        P(),
        P(None, "tp"),
        P(None, "tp"),
        P(None, "tp"),
        P(),
        P(None, "tp"),
        P("tp"),
        P(),
        P(EP, "tp", None, None),
        P("tp", None),
        P(),
        P(EP, None),
        P(EP, None),
        P(EP, None, "tp"),
        P(EP, None, "tp"),
        P(EP, "tp", None),
        P(EP, "tp"),
        P(EP, "tp"),
        P("tp", EP),
        P(),
    )
    return jax.shard_map(
        shards, mesh=split, in_specs=placed, out_specs=P(EP, "tp"), check_vma=False
    )
```

```python
import jax
import jax.numpy as jnp
from jax import lax
from jax.sharding import Mesh
from jax.sharding import PartitionSpec as P

from jax.experimental import pallas as pl
from jax.experimental.pallas import tpu as pltpu

DK = 128
TOPK = 6
EP = ("ep_0", "ep_1", "ep_2")
PLANE = ("ep_1", "ep_2")
CAP = 2


EPS = 1e-06


SWAP = [(0, 1), (1, 0)]


def swapped(array):
    return lax.ppermute(array, "tp", SWAP)


def half_of(array, index, dim):
    width = array.shape[dim] // 2
    return lax.dynamic_slice_in_dim(array, index * width, width, dim)


def exchanged(array, axis):
    return lax.all_to_all(array, axis, split_axis=0, concat_axis=0, tiled=True)


def rms_scale(values_in, gain):
    widened = values_in.astype(jnp.float32)
    return (
        widened
        * lax.rsqrt(jnp.mean(widened * widened, axis=-1, keepdims=True) + EPS)
        * gain.astype(jnp.float32)
    )


def dot(a, b, dims=((1,), (0,))):
    return lax.dot_general(a, b, (dims, ((), ())), preferred_element_type=jnp.float32)


FAR = pl.BlockSpec(memory_space=pl.ANY)
NEAR = pl.BlockSpec(memory_space=pltpu.VMEM)
SMALL = pltpu.CompilerParams(vmem_limit_bytes=32 * 2**20)


def in_vmem(array):
    return pltpu.with_memory_space_constraint(array, pltpu.VMEM)


def placed_lanes(tile, lane, source, target, size):
    shift = (target - source) % 128
    turned = tile if shift == 0 else pltpu.roll(tile, shift, 1)
    return jnp.where((lane >= target) & (lane < target + size), turned, 0.0)


def attend(*refs):
    far, result, side, near, done = refs[:16], refs[16], refs[17], refs[18:34], refs[34]
    copies = [pltpu.make_async_copy(far[k], near[k], done.at[k]) for k in range(16)]
    for copy in copies:
        copy.start()
    (
        tokens, gain, query_weight, decay_down, key_weight, decay_up, decay_bias, value_weight,
        ids, weights, dense_gate, dense_up, dense_down, state, head_gain, out_weight,
    ) = near
    count = tokens.shape[0]
    copies[0].wait()
    copies[1].wait()
    normed = rms_scale(tokens[...], gain[...][None, :]).astype(jnp.bfloat16)
    copies[2].wait()
    query = dot(normed, query_weight[...]) * DK ** (-0.5)
    copies[3].wait()
    decay_low = dot(normed, decay_down[...], ((1,), (1,))).astype(jnp.bfloat16)
    copies[4].wait()
    keys = dot(normed, key_weight[...])
    copies[5].wait()
    copies[6].wait()
    decay_pre = dot(decay_low, decay_up[...]) + decay_bias[...][None, :]
    log_decay = jnp.minimum(decay_pre, 0.0) - jnp.log1p(jnp.exp(-jnp.abs(decay_pre)))
    columns = jnp.transpose(query * jnp.exp(log_decay / 16.0))
    copies[7].wait()
    values = dot(normed, value_weight[...])

    for k in range(8, 13):
        copies[k].wait()
    lane = lax.broadcasted_iota(jnp.int32, (8, 128), 1)
    line = lax.broadcasted_iota(jnp.int32, (8, 128), 0)
    shares = weights[...] / jnp.sum(weights[...], axis=1, keepdims=True)
    chosen = jnp.zeros((8, 128), jnp.float32)
    share = jnp.zeros((8, 128), jnp.float32)
    for k in range(TOPK):
        named = ids[:, k : k + 1] == lane
        chosen = chosen + jnp.where(named, 1.0, 0.0)
        share = share + jnp.where(named, shares[:, k : k + 1], 0.0)
    place = jnp.where(chosen > 0.0, 1.0, 0.0)
    for k in range(1, count):
        place = place + jnp.where(line >= k, pltpu.roll(chosen, k, 0), 0.0)
    place = place * chosen
    share_high = share.astype(jnp.bfloat16).astype(jnp.float32)
    share_low = share - share_high
    for z in range(8):
        tiles = []
        for part in range(2):
            tile = jnp.zeros((8, 128), jnp.float32)
            for m, matrix in enumerate((dense_gate, dense_up, dense_down)):
                start = 128 * (z // 4)
                piece = matrix[...].astype(jnp.float32)[8 * part : 8 * part + 8, start : start + 128]
                tile = tile + placed_lanes(piece, lane, 32 * (z % 4), 32 * m, 32)
            tiles.append(tile)
        tiles[0] = tiles[0] + placed_lanes(place, lane, 16 * z, 96, 16)
        tiles[0] = tiles[0] + placed_lanes(share_high, lane, 16 * z, 112, 16)
        tiles[1] = tiles[1] + placed_lanes(share_low, lane, 16 * z, 96, 16)
        side[z] = jnp.concatenate(tiles, axis=1).astype(jnp.bfloat16)

    copies[13].wait()
    read = [
        jnp.sum(columns[:, k : k + 1] * state[k], axis=0, keepdims=True) for k in range(count)
    ]
    head = jnp.concatenate(read, axis=0) + jnp.sum(query * keys, axis=1, keepdims=True) * values
    copies[14].wait()
    head = rms_scale(head, head_gain[...][None, :]).astype(jnp.bfloat16)
    copies[15].wait()
    result[...] = dot(head, out_weight[...]).astype(jnp.bfloat16)


def attended(*held):
    tokens = held[0]
    return pl.pallas_call(
        attend,
        out_shape=(
            pltpu.VMEM(tokens.shape, jnp.bfloat16),
            pltpu.VMEM((8, 8, 256), jnp.bfloat16),
        ),
        in_specs=[FAR] * 16,
        out_specs=(NEAR, NEAR),
        scratch_shapes=[pltpu.VMEM(a.shape, a.dtype) for a in held]
        + [pltpu.SemaphoreType.DMA((16,))],
        name="attend",
    )(*held)


def assemble(core, tokens, mine, theirs, gain, side, first, own, block, done):
    sides = pltpu.make_async_copy(side, first.at[:, :, pl.ds(1024, 256)], done.at[8])
    sides.start()
    both = mine[...].astype(jnp.float32) + theirs[...].astype(jnp.float32)
    residual = (tokens[...].astype(jnp.float32) + both).astype(jnp.bfloat16)
    normed = rms_scale(residual, gain[...][None, :])
    half = normed.shape[1] // 2
    first_half = core[0] == 0
    block[...] = jnp.where(first_half, normed[:, :half], normed[:, half:]).astype(jnp.bfloat16)
    copies = [
        pltpu.make_async_copy(block, first.at[z, :, pl.ds(0, 1024)], done.at[z]) for z in range(8)
    ]
    for copy in copies:
        copy.start()
    wide = residual.astype(jnp.float32)
    own[...] = jnp.where(first_half, wide[:, :half], wide[:, half:])
    for copy in copies:
        copy.wait()
    sides.wait()


def assembled(core, tokens, mine, theirs, gain, side):
    rows, width = tokens.shape
    return pl.pallas_call(
        assemble,
        out_shape=(
            jax.ShapeDtypeStruct((8, rows, width // 2 + 256), jnp.bfloat16),
            pltpu.VMEM((rows, width // 2), jnp.float32),
        ),
        in_specs=[pl.BlockSpec(memory_space=pltpu.SMEM)] + [NEAR] * 5,
        out_specs=(FAR, NEAR),
        scratch_shapes=[
            pltpu.VMEM((rows, width // 2), jnp.bfloat16),
            pltpu.SemaphoreType.DMA((9,)),
        ],
        compiler_params=SMALL,
        name="assemble",
    )(
        core, in_vmem(tokens), in_vmem(mine), in_vmem(theirs),
        in_vmem(gain), in_vmem(side),
    )


def route(line, second, copy, weights):
    planes, depth, _ = second.shape
    half = line.shape[1] - 256
    tiles = [
        line[:, half + 128 * k : half + 128 * (k + 1)].astype(jnp.float32) for k in range(2)
    ]
    lane = lax.broadcasted_iota(jnp.int32, (8, 128), 1)
    for which in range(3):
        for parity in range(2):
            parts = []
            for tile in tiles:
                part = jnp.zeros((8, 128), jnp.float32)
                for quarter in range(4):
                    z = 2 * quarter + parity
                    part = part + placed_lanes(
                        tile[8 * z : 8 * z + 8], lane, 32 * which, 32 * quarter, 32
                    )
                parts.append(part)
            start = 256 * which + 128 * parity
            weights[:, start : start + 128] = jnp.concatenate(parts, axis=0).astype(jnp.bfloat16)
    second[:, :, half:] = jnp.broadcast_to(weights[...][None], (planes, depth, 768))
    copy[...] = line[:, :half]
    marks = line[:, half : half + 128]
    count = planes * depth
    row = lax.broadcasted_iota(jnp.int32, (count, 128), 0)
    lane = lax.broadcasted_iota(jnp.int32, (count, 128), 1)
    spread = jnp.where(lane == 96 + row // depth, 1.0, 0.0).astype(jnp.bfloat16)
    place = dot(spread, marks, ((1,), (1,)))
    row, lane = row[:, : line.shape[0]], lane[:, : line.shape[0]]
    taken = (place == (1 + row % CAP).astype(jnp.float32)) & (row // CAP % 8 == lane // 8)
    taken = jnp.where(taken, 1.0, 0.0).astype(jnp.bfloat16)
    second[:, :, :half] = (
        dot(taken, line[:, :half]).astype(jnp.bfloat16).reshape(planes, depth, half)
    )


def routed_rows(line, planes):
    half = line.shape[1] - 256
    return pl.pallas_call(
        route,
        out_shape=(
            pltpu.VMEM((planes, 16, half + 768), jnp.bfloat16),
            pltpu.VMEM((line.shape[0], half), jnp.bfloat16),
        ),
        in_specs=[NEAR],
        out_specs=(NEAR, NEAR),
        scratch_shapes=[pltpu.VMEM((16, 768), jnp.bfloat16)],
        compiler_params=SMALL,
        name="route",
    )(in_vmem(line))


def widen(core, arrived, gate, up, far, pre, sent):
    planes, depth, _ = arrived.shape
    half, wide = far.shape
    units = wide // 2
    rows = arrived[:, :, :half].reshape(planes * depth, half)
    start = pl.multiple_of(core[0] * half, half)
    there = dot(rows, far[...])
    here = [dot(rows, matrix[pl.ds(start, half), :]) for matrix in (gate, up)]
    parts = (here[0], there[:, :units], here[1], there[:, units:])
    for k in range(4):
        pre[:, k * units : (k + 1) * units] = parts[k]
        sent[:, k * units : (k + 1) * units] = parts[k ^ 1].astype(jnp.bfloat16)


def widened(core, arrived, gate, up, far):
    slots, wide = arrived.shape[0] * arrived.shape[1], 2 * far.shape[1]
    return pl.pallas_call(
        widen,
        out_shape=(
            pltpu.VMEM((slots, wide), jnp.float32),
            pltpu.VMEM((slots, wide), jnp.bfloat16),
        ),
        in_specs=[pl.BlockSpec(memory_space=pltpu.SMEM)] + [NEAR] * 4,
        out_specs=(NEAR, NEAR),
        compiler_params=SMALL,
        name="widen",
    )(core, *[in_vmem(a) for a in (arrived, gate, up, far)])


def narrow(core, pre, came, down, far, result):
    units = far.shape[0]
    planes, depth, half = result.shape
    start = pl.multiple_of(core[0] * half, half)
    near = down[:, pl.ds(start, half)]
    total = pre[...] + came[...].astype(jnp.float32)
    gate = total[:, : 2 * units]
    hidden = (gate / (1.0 + jnp.exp(-gate)) * total[:, 2 * units :]).astype(jnp.bfloat16)
    out = dot(hidden[:, :units], near) + dot(hidden[:, units:], far[...])
    result[...] = out.astype(jnp.bfloat16).reshape(planes, depth, half)


def narrowed(core, pre, came, down, far, planes):
    shape = (planes, pre.shape[0] // planes, far.shape[1])
    return pl.pallas_call(
        narrow,
        out_shape=pltpu.VMEM(shape, jnp.bfloat16),
        in_specs=[pl.BlockSpec(memory_space=pltpu.SMEM)] + [NEAR] * 4,
        out_specs=NEAR,
        compiler_params=SMALL,
        name="narrow",
    )(core, *[in_vmem(a) for a in (pre, came, down, far)])


def matrix_of(arrived, m, half):
    planes, depth, _ = arrived.shape
    starts = [half + 256 * m + 128 * p for p in range(2)]
    blocks = [arrived[:, :, at : at + 128].reshape(planes * depth, 128) for at in starts]
    return jnp.concatenate(blocks, axis=0)


def added(source, marks, arrived, first, gate, up, pre):
    count, half = source.shape
    quarter = half // 2
    group = lax.broadcasted_iota(jnp.int32, (count, 128), 1) // 32
    both = jnp.concatenate([matrix_of(arrived, m, half) for m in range(2)], axis=1)
    wide = source.astype(jnp.float32) * marks[...].astype(jnp.float32)[None, :]
    pre = pre + jnp.sum(wide, axis=1, keepdims=True)
    for k in range(2):
        part = dot(source[:, k * quarter : (k + 1) * quarter], both)
        gate = gate + jnp.where(group == first + k, part[:, :128], 0.0)
        up = up + jnp.where(group == first + k, part[:, 128:], 0.0)
    return gate, up, pre


def branch_in(core, arrived, line, marks, gate, up, pre, high, low):
    planes, depth, _ = arrived.shape
    count, half = line.shape[0], line.shape[1] - 256
    zero = jnp.zeros((count, 128), jnp.float32)
    gate[...], up[...], pre[...] = added(
        line[:, :half], marks, arrived, 2 * core[0], zero, zero, zero
    )

    slots = planes * depth
    row = lax.broadcasted_iota(jnp.int32, (slots, 128), 0)
    lane = lax.broadcasted_iota(jnp.int32, (slots, 128), 1)

    def over_slots(start, tile):
        spread = jnp.where(lane == start + row // depth, 1.0, 0.0).astype(jnp.bfloat16)
        return dot(spread, line[:, half + 128 * tile : half + 128 * (tile + 1)], ((1,), (1,)))

    place, share = over_slots(96, 0), over_slots(112, 0) + over_slots(96, 1)
    row, lane = row[:, :count], lane[:, :count]
    taken = (place == (1 + row % CAP).astype(jnp.float32)) & (row // CAP % 8 == lane // 8)
    weighing = jnp.where(taken, share, 0.0)
    upper = weighing.astype(jnp.bfloat16)
    high[...] = upper
    low[...] = (weighing - upper.astype(jnp.float32)).astype(jnp.bfloat16)


def branch_out(core, arrived, rest, marks, gate_own, up_own, pre_own, keep, sent):
    count, half = rest.shape
    quarter = half // 2
    group = lax.broadcasted_iota(jnp.int32, (count, 128), 1) // 32
    gate, up, pre = added(
        rest[...], marks, arrived, 2 - 2 * core[0], gate_own[...], up_own[...], pre_own[...]
    )

    def folded(total):
        return total + sum(pltpu.roll(total, 32 * k, 1) for k in range(1, 4))

    gate = folded(gate)
    hidden = gate / (1.0 + jnp.exp(-gate)) * folded(up)
    branch = 1.0 / (1.0 + jnp.exp(-pre[:, :1]))
    down = matrix_of(arrived, 2, half)
    for target, first in ((sent, 2 - 2 * core[0]), (keep, 2 * core[0])):
        for k in range(2):
            units = jnp.where(group == first + k, hidden, 0.0).astype(jnp.bfloat16)
            target[:, k * quarter : (k + 1) * quarter] = (
                branch * dot(units, down, ((1,), (1,)))
            ).astype(jnp.bfloat16)


def on_core(kernel, shapes, core, *arrays):
    return pl.pallas_call(
        kernel,
        out_shape=tuple(pltpu.VMEM(shape, kind) for shape, kind in shapes),
        in_specs=[pl.BlockSpec(memory_space=pltpu.SMEM)] + [NEAR] * len(arrays),
        out_specs=(NEAR,) * len(shapes),
        compiler_params=SMALL,
    )(core, *[in_vmem(a) for a in arrays])


def shards(
    tokens,
    first_gain,
    query_weight,
    key_weight,
    value_weight,
    decay_down,
    decay_up,
    decay_bias,
    head_gain,
    recurrent_state,
    out_weight,
    second_gain,
    expert_ids,
    route_weights,
    expert_gate,
    expert_up,
    expert_down,
    dense_gate,
    dense_up,
    dense_down,
    branch_gate,
):
    rows_dev, width = tokens.shape
    core = lax.axis_index("tp")
    lines = lax.axis_size("ep_0")
    plane = lax.axis_size(PLANE)
    half = width // 2
    partial_value, side = attended(
        tokens, first_gain, query_weight, decay_down.T, key_weight, decay_up, decay_bias,
        value_weight, expert_ids, route_weights, dense_gate, dense_up, dense_down.T,
        recurrent_state[:, 0], head_gain, out_weight,
    )
    which = core.reshape(1).astype(jnp.int32)
    first, own_half = assembled(
        which, tokens, partial_value, swapped(partial_value), second_gain, side
    )
    first, gate, up, down = lax.optimization_barrier(
        (first, expert_gate[0], expert_up[0], expert_down[0])
    )
    line = exchanged(first, "ep_0")
    line = line.reshape(lines * rows_dev, half + 256)
    given = jnp.concatenate([half_of(gate, 1 - core, 0), half_of(up, 1 - core, 0)], axis=1)
    far_in = swapped(given)
    mark_own = half_of(branch_gate, core, 0)
    mark_rest = half_of(branch_gate, 1 - core, 0)
    far_down = swapped(half_of(down, 1 - core, 1))
    line, far_in, far_down, gate, up, down, mark_own, mark_rest = lax.optimization_barrier(
        (line, far_in, far_down, gate, up, down, mark_own, mark_rest)
    )
    second, line_half = routed_rows(line, plane)
    arrived = exchanged(second, PLANE)
    arrived, line_half = lax.optimization_barrier((arrived, line_half))
    slots = plane * lines * CAP
    rest = swapped(line_half)
    pre, sent = widened(which, arrived, gate, up, far_in)
    came = swapped(sent)
    count = lines * rows_dev
    *sums, weigh_high, weigh_low = on_core(
        branch_in,
        [((count, 128), jnp.float32)] * 3 + [((slots, count), jnp.bfloat16)] * 2,
        which, arrived, line, mark_own,
    )
    keep, given_part = on_core(
        branch_out, [((count, half), jnp.bfloat16)] * 2,
        which, arrived, rest, mark_rest, *sums,
    )
    given_part = swapped(given_part)
    summed = narrowed(which, pre, came, down, far_down, plane)
    dense = keep.astype(jnp.float32) + given_part.astype(jnp.float32)
    summed, dense, weigh_high, weigh_low = lax.optimization_barrier(
        (summed, dense, weigh_high, weigh_low)
    )
    came_back = exchanged(summed, PLANE)

    def combined(part):
        return lax.dot_general(
            part,
            came_back.reshape(slots, half),
            (((0,), (0,)), ((), ())),
            preferred_element_type=jnp.float32,
        )

    third = (combined(weigh_high) + combined(weigh_low) + dense).astype(jnp.bfloat16)
    parts = exchanged(third.reshape(lines, rows_dev, half), "ep_0")
    return (own_half + parts.astype(jnp.float32).sum(axis=0)).astype(jnp.bfloat16)


def solution(mesh):
    split = Mesh(mesh.devices.reshape(8, 4, 4, mesh.shape["tp"]), ("ep_0", "ep_1", "ep_2", "tp"))
    placed = (
        P(EP, None),
        P(),
        P(None, "tp"),
        P(None, "tp"),
        P(None, "tp"),
        P(),
        P(None, "tp"),
        P("tp"),
        P(),
        P(EP, "tp", None, None),
        P("tp", None),
        P(),
        P(EP, None),
        P(EP, None),
        P(EP, None, "tp"),
        P(EP, None, "tp"),
        P(EP, "tp", None),
        P(EP, "tp"),
        P(EP, "tp"),
        P("tp", EP),
        P(),
    )
    return jax.shard_map(
        shards, mesh=split, in_specs=placed, out_specs=P(EP, "tp"), check_vma=False
    )
```
